256 devices in a mesh: ep: 16 (over y, x), tp: 16 (over z, core).
Axes of the slice: x: 4, y: 4, z: 8, core: 2. Of those that a mesh axis runs over, the one named last changes fastest.
Arguments:
- tokens: bfloat16 [4096, 4096], P('ep'), may hold values from -6 to 6
- cotangent: bfloat16 [4096, 4096], P('ep'), may hold values from -6 to 6
- routing: int32 [4096, 2], P('ep'), may hold values from 0 to 15, all different within a row; in each aligned block of 256 rows (0 to 255, 256 to 511, ...) at most 40 rows name the same one
- group_gate: float32 [4096], P('ep'), may hold values from 0.2 to 1
- inner_gate: float32 [4096, 2], P('ep'), may hold values from 0.1 to 0.9
- w_gate: bfloat16 [16, 4096, 2048], P('ep', None, 'tp'), may hold values from -0.09375 to 0.09375
- w_up: bfloat16 [16, 4096, 2048], P('ep', None, 'tp'), may hold values from -0.09375 to 0.09375
- w_down: bfloat16 [16, 2048, 4096], P('ep', 'tp'), may hold values from -0.125 to 0.125
Outputs:
- token_grad: bfloat16 [4096, 4096], P('ep', 'tp')
- group_grad: float32 [4096], P('ep')
- inner_grad: float32 [4096, 2], P('ep')
- gate_weight_grad: bfloat16 [16, 4096, 2048], P('ep', None, 'tp')
- up_weight_grad: bfloat16 [16, 4096, 2048], P('ep', None, 'tp')
- down_weight_grad: bfloat16 [16, 2048, 4096], P('ep', 'tp')
The draws below stay inside these ranges and needn't reach their ends.
Inputs may be any that keep to these rules, and one draw needn't show every extreme that they name: `routing`: each row names 2 different experts. Among the rows of one device (aligned blocks of 256 rows) no expert is named more than 40 times, and in every draw some expert is named exactly 40 times in some block.
All inputs are finite; a program needn't handle non-finite values.
Results may differ from the reference program's by a relative error of at most 0.02.
Values may be sent and summed in bfloat16 or wider, within the bound.
No kernel may reach another device: no remote copies, remote signals or barrier semaphores. Data moves between devices by JAX's collectives and lax.ppermute only.
A program may use at most 128 MiB of HBM per device.

```python
import math
import jax
import jax.numpy as jnp
import numpy as np
from jax import lax

D = 4096
FF = 2048
TOP = 2
TOK_DEV = 256
EXPERTS = 16
CAP = 40
TOKENS = 4096
N_EP = 16
N_TP = 16


def block_levels(rng, dims, split, least, high):
    factor_of, own = 1.0, jax.random.fold_in(rng, 6)
    for dim, blocks in split:
        draws = jnp.exp(jax.random.uniform(jax.random.fold_in(own, dim), (blocks,), jnp.float32, least / len(split), high / len(split)))
        factor_of = factor_of * jnp.repeat(draws, dims[dim] // blocks).reshape([-1 if axis == dim else 1 for axis in range(len(dims))])
    return factor_of


def deal_out(stream_key, own, number, rows, number_of, top, bound, lean):
    order = jax.random.permutation(stream_key, number_of)
    crowded, usual = load_shares(number_of, rows * top, bound, lean, True), load_shares(number_of, rows * top, bound, lean, False)
    places = jnp.arange(number_of)

    def named(tallies, turn):
        used = int((tallies > 0).sum())
        fixed = max(1, used // 4)
        passed = fixed + (places - fixed + turn * (used - fixed)) % max(1, number_of - fixed)
        return jnp.zeros((number_of,), jnp.int32).at[order[jnp.where(places < fixed, places, passed)]].set(jnp.asarray(tallies, jnp.int32))

    tallies = jnp.where(number % 4 == 0, named(crowded, number // 4), named(usual, number - number // 4 - 1))
    mixed = jax.random.permutation(jax.random.fold_in(own, 3), number_of)
    donor, taker = mixed[0:number_of // 2 * 2:2], mixed[1:number_of // 2 * 2:2]
    margin = jnp.minimum(tallies[donor] - 1, bound - tallies[taker]) // 2
    margin = jnp.where((donor == order[0]) | (taker == order[0]) | (tallies[taker] == 0), 0, jnp.maximum(margin, 0))
    passed = jax.random.randint(jax.random.fold_in(own, 4), (number_of // 2,), 0, 1 << 20) % (margin + 1)
    tallies = tallies.at[donor].add(-passed).at[taker].add(passed)
    members = jnp.searchsorted(jnp.cumsum(tallies), jnp.arange(rows * top), side="right").astype(jnp.int32)
    grid = members.reshape(top, rows).T
    grid = grid[jax.random.permutation(jax.random.fold_in(own, 1), rows)]
    turn = jax.random.randint(jax.random.fold_in(own, 2), (rows, 1), 0, top)
    return jnp.take_along_axis(grid, (jnp.arange(top)[None, :] + turn) % top, axis=1)


def load_shares(amount, total, bound, skew, full):
    portions = [(1 << 20) // math.isqrt(standing ** skew) + 1 for standing in range(1, amount + 1)]
    largest = bound if full else min(bound, max(-(-total // amount), total * portions[0] // sum(portions)))
    least = 1 if total - largest >= amount - 1 else 0
    given, rest = [largest] + [least] * (amount - 1), total - largest - least * (amount - 1)
    while rest > 0:
        movable = [i for i in range(1, amount) if given[i] < largest] or [i for i in range(1, amount) if given[i] < bound]
        mass, budget = sum([portions[i] for i in movable]), rest
        for i in movable:
            more = min(bound - given[i], max(1, budget * portions[i] // mass), rest)
            given[i] = given[i] + more
            rest = rest - more
    return np.array(given)


def centred(own_key, shape, deviation, limit, split=(), kind=jnp.bfloat16):
    drawn = deviation * jax.random.normal(own_key, shape, jnp.float32)
    if split:
        drawn = drawn * block_levels(own_key, shape, split, -0.22, 0.18)
    return jnp.clip(drawn, -limit, limit).astype(kind)


def setup_inputs(seed: int = 0) -> dict:
    seeds = jax.random.split(jax.random.key(seed), 9)
    tokens = centred(seeds[0], (TOKENS, D), 1.0, 6.0, ((0, 16),))
    cotangent = centred(seeds[1], (TOKENS, D), 1.0, 6.0, ((0, 16),))
    routing_keys = jax.random.split(jax.random.fold_in(seeds[2], 1), TOKENS // TOK_DEV)
    routing_turns = jax.random.permutation(jax.random.fold_in(seeds[2], 3), TOKENS // TOK_DEV)
    routing = jax.vmap(lambda own, number: deal_out(jax.random.fold_in(seeds[2], 2), own, number, TOK_DEV, EXPERTS, TOP, CAP, 2))(routing_keys, routing_turns).reshape((TOKENS, TOP))
    group_gate = jnp.clip(0.2 + 0.8 * jax.random.uniform(seeds[3], (TOKENS,), jnp.float32) ** block_levels(seeds[3], (TOKENS,), ((0, 16),), -0.2, 0.2), 0.2, 1.0)
    inner_gate = jnp.clip(0.1 + 0.79999997 * jax.random.uniform(seeds[4], (TOKENS, TOP), jnp.float32) ** block_levels(seeds[4], (TOKENS, TOP), ((0, 16),), -0.2, 0.2), 0.1, 0.9)
    w_gate = centred(seeds[5], (EXPERTS, D, FF), D ** -0.5, 0.09375, ((0, 16), (2, 16)))
    w_up = centred(seeds[6], (EXPERTS, D, FF), D ** -0.5, 0.09375, ((0, 16), (2, 16)))
    w_down = centred(seeds[7], (EXPERTS, FF, D), FF ** -0.5, 0.125, ((0, 16), (1, 16)))
    return dict(tokens=tokens, cotangent=cotangent, routing=routing, group_gate=group_gate, inner_gate=inner_gate, w_gate=w_gate, w_up=w_up, w_down=w_down)


def expert_backward(packed):
    rows_in, cot_rows, row_weight, gate_weight, up_weight, down_weight = packed
    gate_pre = jnp.dot(rows_in, gate_weight, preferred_element_type=jnp.float32)
    up_pre = jnp.dot(rows_in, up_weight, preferred_element_type=jnp.float32)
    sigmoid_gate = jax.nn.sigmoid(gate_pre)
    silu_gate = gate_pre * sigmoid_gate
    hidden = (silu_gate * up_pre).astype(jnp.bfloat16)
    scaled_cot = (row_weight[:, None] * cot_rows.astype(jnp.float32)).astype(jnp.bfloat16)
    down_grad = jnp.dot(hidden.T, scaled_cot, preferred_element_type=jnp.float32).astype(jnp.bfloat16)
    grad_hidden = jnp.dot(cot_rows, down_weight.T, preferred_element_type=jnp.float32)
    scores = jnp.sum(grad_hidden * hidden.astype(jnp.float32), axis=1)
    weighted = row_weight[:, None] * grad_hidden
    grad_gate_in = (weighted * up_pre * sigmoid_gate * (1.0 + gate_pre * (1.0 - sigmoid_gate))).astype(jnp.bfloat16)
    grad_up_in = (weighted * silu_gate).astype(jnp.bfloat16)
    gate_grad = jnp.dot(rows_in.T, grad_gate_in, preferred_element_type=jnp.float32).astype(jnp.bfloat16)
    upper_grad = jnp.dot(rows_in.T, grad_up_in, preferred_element_type=jnp.float32).astype(jnp.bfloat16)
    row_count = rows_in.shape[0]
    model_width = rows_in.shape[1]
    block_units = FF // N_TP
    gate_blocks = grad_gate_in.astype(jnp.float32).reshape(row_count, N_TP, block_units)
    up_blocks = grad_up_in.astype(jnp.float32).reshape(row_count, N_TP, block_units)
    gate_w_blocks = gate_weight.astype(jnp.float32).reshape(model_width, N_TP, block_units)
    up_w_blocks = up_weight.astype(jnp.float32).reshape(model_width, N_TP, block_units)
    partial_rows = (jnp.einsum('rnf,dnf->nrd', gate_blocks, gate_w_blocks, precision=lax.Precision.HIGHEST)
                    + jnp.einsum('rnf,dnf->nrd', up_blocks, up_w_blocks, precision=lax.Precision.HIGHEST))
    rounded_parts = partial_rows.astype(jnp.bfloat16).astype(jnp.float32)
    row_grad = jnp.sum(rounded_parts, axis=0).astype(jnp.bfloat16)
    return gate_grad, upper_grad, down_grad, row_grad, scores


def reference(tokens, cotangent, routing, group_gate, inner_gate, w_gate, w_up, w_down):
    token_count, model_width = tokens.shape
    slots_expert = N_EP * CAP
    total_slots = EXPERTS * slots_expert
    flat_route = routing.reshape(N_EP, TOK_DEV * TOP)
    one_hot = (flat_route[:, :, None] == jnp.arange(EXPERTS, dtype=jnp.int32)[None, None, :]).astype(jnp.int32)
    within = jnp.sum(one_hot * (jnp.cumsum(one_hot, axis=1) - 1), axis=2)
    source = jnp.arange(N_EP, dtype=jnp.int32)[:, None]
    slot_of = (flat_route * slots_expert + source * CAP + within).reshape(-1).astype(jnp.int32)
    token_of = jnp.arange(token_count * TOP, dtype=jnp.int32) // TOP
    combine = (group_gate[:, None] * inner_gate).reshape(-1)
    rows_in = jnp.zeros((total_slots, model_width), jnp.bfloat16).at[slot_of].set(tokens[token_of])
    cot_rows = jnp.zeros((total_slots, model_width), jnp.bfloat16).at[slot_of].set(cotangent[token_of])
    row_weight = jnp.zeros((total_slots,), jnp.float32).at[slot_of].set(combine)
    results = lax.map(expert_backward, (rows_in.reshape(EXPERTS, slots_expert, model_width),
                                        cot_rows.reshape(EXPERTS, slots_expert, model_width),
                                        row_weight.reshape(EXPERTS, slots_expert), w_gate, w_up, w_down))
    gate_grad, upper_grad, down_grad, row_grad, scores = results
    picked = row_grad.reshape(total_slots, model_width)[slot_of].astype(jnp.float32)
    token_grad = jnp.sum(picked.reshape(token_count, TOP, model_width), axis=1).astype(jnp.bfloat16)
    score_of = scores.reshape(total_slots)[slot_of].reshape(token_count, TOP)
    inner_grad = group_gate[:, None] * score_of
    group_grad = jnp.sum(inner_gate * score_of, axis=1)
    return token_grad, group_grad, inner_grad, gate_grad, upper_grad, down_grad
```

```python
import jax
import jax.numpy as jnp
from jax import lax
from jax.experimental import pallas as pl
from jax.experimental.pallas import tpu as pltpu
from jax.sharding import Mesh, PartitionSpec as P


BF = jnp.bfloat16
F32 = jnp.float32
I32 = jnp.int32
UNIT = 512
WIRE = 640
A_UNITS = 5
B_UNITS = 3
WHOLE = pl.BlockSpec(memory_space=pltpu.VMEM)
SCALARS = pl.BlockSpec(memory_space=pltpu.SMEM)


def iota(shape, dim):
    return lax.broadcasted_iota(I32, shape, dim)


def as_bf(mask):
    return jnp.where(mask, 1.0, 0.0).astype(BF)


def mm(a, b, ca=1, cb=0):
    return lax.dot_general(a, b, (((ca,), (cb,)), ((), ())), preferred_element_type=F32)


def fold_matrix():
    o = iota((256, 256), 0)
    i = iota((256, 256), 1)
    return as_bf(((o >> 6) == ((i >> 2) & 3)) & (((o >> 2) & 15) == (i >> 4)) & ((o & 3) == (i & 3)))


def pack_unit(ohm, oht, src, out):
    row = iota((256, 256), 0)
    out[:, :UNIT] = mm(ohm, src[...]).astype(BF)
    tail = jnp.zeros((256, 128), F32)
    for q in range(4):
        tail += mm(jnp.where(((row >> 2) & 3) == q, oht, jnp.zeros_like(oht)), src[:, q * 128 : q * 128 + 128])
    out[:, UNIT:WIRE] = tail.astype(BF)


def pack_a(s_ref, r_ref, x_ref, g_ref, a_ref, rank_ref, ohm_ref, oht_ref):
    @pl.when(pl.program_id(0) == 0)
    def _():
        r = r_ref[...]
        lane = iota((256, 128), 1)
        named = (r[:, 0:1] == lane) | (r[:, 1:2] == lane)
        ti = iota((256, 256), 0)
        tj = iota((256, 256), 1)
        rank = mm(as_bf(tj < ti), as_bf(named))
        rank = jnp.where(named, rank, -1.0)
        rank_ref[...] = rank
        by_expert = mm(rank.astype(BF), as_bf(ti == tj), 0, 0).astype(BF)
        row = iota((256, 128), 0)
        spread = mm(as_bf((row >> 4) == lane), by_expert).astype(I32)
        first = s_ref[1] * 20
        ohm_ref[...] = as_bf(spread == first + (ti & 15))
        oht_ref[...] = as_bf(spread == first + 16 + (ti & 3))

    @pl.when(s_ref[0] == 0)
    def _():
        pack_unit(ohm_ref[...], oht_ref[...], x_ref, a_ref)

    @pl.when(s_ref[0] != 0)
    def _():
        pack_unit(ohm_ref[...], oht_ref[...], g_ref, a_ref)


def pack_b(r_ref, gg_ref, ig_ref, ohm_ref, oht_ref, x_ref, g_ref, bx_ref, bg_ref, wt_ref):
    ohm = ohm_ref[...]
    oht = oht_ref[...]
    pack_unit(ohm, oht, x_ref, bx_ref)
    pack_unit(ohm, oht, g_ref, bg_ref)

    @pl.when(pl.program_id(0) == 0)
    def _():
        r = r_ref[...]
        lane = iota((256, 128), 1)
        row = iota((256, 128), 0)
        comb = gg_ref[...] * ig_ref[...]
        w = jnp.where(r[:, 0:1] == lane, comb[:, 0:1], 0.0) + jnp.where(r[:, 1:2] == lane, comb[:, 1:2], 0.0)
        hi = w.astype(BF)
        lo = (w - hi.astype(F32)).astype(BF)
        own = lane == (row >> 4)

        def picked(oh, part):
            return jnp.sum(jnp.where(own, mm(oh, part), 0.0), axis=1, keepdims=True)

        vals = jnp.where(lane == 0, picked(ohm, hi), 0.0)
        vals = jnp.where(lane == 1, picked(ohm, lo), vals)
        vals = jnp.where(lane == 2, picked(oht, hi), vals)
        vals = jnp.where(lane == 3, picked(oht, lo), vals)
        wt_ref[...] = vals.astype(BF)


def expert_kernel(s_ref, a_ref, z1_ref, z2_ref, bx_ref, bg_ref, wt_ref, wcat_ref, wd_ref,
                  x_out, g_out, c_out, hid_out, gown_out, gpar_out, p1_out, p2_out):
    fold = fold_matrix()
    fold0 = fold[0:64, :]
    lane = iota((256, 128), 1)
    row = iota((256, 128), 0)

    def unpack(buf, off, dst, u):
        dst[0:256, u * UNIT : (u + 1) * UNIT] = buf[:, off : off + UNIT]
        t = mm(fold, buf[:, off + UNIT : off + WIRE]).astype(BF)
        for q in range(4):
            dst[256:320, u * UNIT + q * 128 : u * UNIT + q * 128 + 128] = t[q * 64 : q * 64 + 64, :]

    def unpack_z(dst, u):
        off = u * WIRE
        dst[0:128, u * UNIT : (u + 1) * UNIT] = z1_ref[:, off : off + UNIT]
        dst[128:256, u * UNIT : (u + 1) * UNIT] = z2_ref[:, off : off + UNIT]
        t = mm(fold[:, 0:128], z1_ref[:, off + UNIT : off + WIRE])
        t = (t + mm(fold[:, 128:256], z2_ref[:, off + UNIT : off + WIRE])).astype(BF)
        for q in range(4):
            dst[256:320, u * UNIT + q * 128 : u * UNIT + q * 128 + 128] = t[q * 64 : q * 64 + 64, :]

    @pl.when(s_ref[0] == 0)
    def _():
        for u in range(A_UNITS):
            unpack(a_ref, u * WIRE, x_out, u)
            unpack_z(g_out, u)

    @pl.when(s_ref[0] != 0)
    def _():
        for u in range(A_UNITS):
            unpack(a_ref, u * WIRE, g_out, u)
            unpack_z(x_out, u)

    for u in range(B_UNITS):
        unpack(bx_ref, u * WIRE, x_out, A_UNITS + u)
        unpack(bg_ref, u * WIRE, g_out, A_UNITS + u)

    wt = wt_ref[...]
    wt_f = wt.astype(F32)
    c_main = wt_f[:, 0:1] + wt_f[:, 1:2]
    wt_t = mm(fold0, wt)
    c_tail = wt_t[:, 2:3] + wt_t[:, 3:4]

    pre = mm(x_out[...], wcat_ref[...])
    gh = mm(g_out[...], wd_ref[...], 1, 1)

    def activations(at, count, c):
        gate_pre = pre[at : at + count, 0:256]
        up_pre = pre[at : at + count, 256:512]
        g = gh[at : at + count, :]
        sig = jax.nn.sigmoid(gate_pre)
        silu = gate_pre * sig
        hid = (silu * up_pre).astype(BF)
        score = jnp.sum(g * hid.astype(F32), axis=1, keepdims=True)
        weighted = c * g
        ggi = (weighted * up_pre * sig * (1.0 + gate_pre * (1.0 - sig))).astype(BF)
        gui = (weighted * silu).astype(BF)
        hid_out[at : at + count, :] = hid
        gown_out[at : at + count, 0:128] = ggi[:, 0:128]
        gown_out[at : at + count, 128:256] = gui[:, 0:128]
        gpar_out[at : at + count, 0:128] = ggi[:, 128:256]
        gpar_out[at : at + count, 128:256] = gui[:, 128:256]
        c_out[at : at + count, :] = jnp.broadcast_to(c, (count, 128))
        hi = score.astype(BF)
        lo = score - hi.astype(F32)
        return jnp.concatenate([ggi, gui], axis=1), hi.astype(F32), lo

    in_main, hi_m, lo_m = activations(0, 256, c_main)
    in_tail, hi_t, lo_t = activations(256, 64, c_tail)
    ins = jnp.concatenate([in_main, in_tail], axis=0)

    lane_t = iota((64, 128), 1)
    tails = jnp.where(lane_t == 2, hi_t, jnp.where(lane_t == 3, lo_t, 0.0)).astype(BF)
    vals = jnp.where(lane == 0, hi_m, jnp.where(lane == 1, lo_m, 0.0)) + mm(fold0, tails, 0, 0)
    ti = iota((128, 128), 0)
    tl = iota((128, 128), 1)
    spread = mm(vals.astype(BF), as_bf((tl & 3) == ti))
    spread = jnp.where((lane >> 2) == (row >> 4), spread, 0.0).astype(BF)
    sr = iota((16, 256), 0)
    sl = iota((16, 256), 1)
    scores = mm(as_bf((sl & 15) == sr), spread).astype(BF)

    z = s_ref[2]
    for k in range(8):
        dest = lax.rem(z + k, 8)
        at = pl.multiple_of(dest * 512, 512)
        w0 = wcat_ref[pl.ds(at + 128, 128), :]
        w1 = wcat_ref[pl.ds(at + 384, 128), :]
        part = mm(ins, jnp.concatenate([w0, w1], axis=0), 1, 1).astype(BF)
        p2_out[k, 0:320, :] = part
        p2_out[k, 320:336, 0:128] = scores
        p2_out[k, 320:336, 128:256] = jnp.zeros((16, 128), BF)

    for c in range(2):
        for u in range(2):
            tail_parts = []
            for h in range(2):
                at = (4 * u + 2 * h) * 512 + c * 256
                w = jnp.concatenate([wcat_ref[at : at + 128, :], wcat_ref[at + 512 : at + 640, :]], axis=0)
                part = mm(ins, w, 1, 1).astype(BF)
                for b in range(16):
                    p1_out[2 * b + c, :, u * WIRE + h * 256 : u * WIRE + h * 256 + 256] = part[16 * b : 16 * b + 16, :]
                tail_parts += [part[256:320, 0:128], part[256:320, 128:256]]
            folded = mm(fold, jnp.concatenate(tail_parts, axis=0), 0, 0).astype(BF)
            for b in range(16):
                p1_out[2 * b + c, :, u * WIRE + UNIT : (u + 1) * WIRE] = folded[16 * b : 16 * b + 16, :]


def slot_masks(r_ref, rank_ref, k):
    r = r_ref[...]
    lane = iota((256, 128), 1)
    expert = r[:, k : k + 1]
    rank = jnp.sum(jnp.where(lane == expert, rank_ref[...], 0.0), axis=1, keepdims=True).astype(I32)
    slot = iota((256, 512), 1)
    here = (slot >> 5) == expert
    left = rank - 20 * ((slot >> 4) & 1)
    return here, left, slot


def combine_kernel(s_ref, r_ref, rank_ref, r1_ref, out_ref, acc_ref):
    masks = [slot_masks(r_ref, rank_ref, k) for k in range(2)]

    def either(test):
        a, b = [here & test(left, slot) for here, left, slot in masks]
        return as_bf(a | b)

    main = either(lambda left, slot: left == (slot & 15))
    tails = [
        either(lambda left, slot, q=q: (left == 16 + (slot & 3)) & (((slot >> 2) & 3) == q)) for q in range(4)
    ]
    for u in range(2):
        full = mm(main, r1_ref[:, u * WIRE : u * WIRE + UNIT])
        tail = r1_ref[:, u * WIRE + UNIT : (u + 1) * WIRE]
        for q in range(4):
            acc_ref[:, u * UNIT + q * 128 : u * UNIT + q * 128 + 128] = (
                full[:, q * 128 : q * 128 + 128] + mm(tails[q], tail)
            ).astype(BF)
    z = s_ref[2]
    for k in range(8):
        at = pl.multiple_of(lax.rem(z + k, 8) * 128, 128)
        out_ref[k, :, :] = acc_ref[:, pl.ds(at, 128)]


def middle_kernel(*refs):
    own, others, out_ref = refs[0], refs[1:8], refs[8]
    total = own[...].astype(F32)
    for o in others:
        total += o[...].astype(F32)
    fold0 = fold_matrix()[0:64, :]
    rows = total[0:320, :].astype(BF)
    tails = mm(fold0, rows[256:320, :], 0, 0).astype(BF)
    s = total[320:336, 0:128]
    lane16 = iota((16, 128), 1)
    both = s + pltpu.roll(s, 127, 1)
    hi = both.astype(BF).astype(F32)
    lo = both - hi
    final = jnp.where((lane16 & 1) == 0, hi, pltpu.roll(lo, 1, 1)).astype(BF)
    er = iota((256, 16), 0)
    ec = iota((256, 16), 1)
    spread = mm(as_bf((er & 15) == ec), final)
    lane = iota((256, 128), 1)
    row = iota((256, 128), 0)
    spread = jnp.where((lane >> 2) == (row >> 4), spread, 0.0).astype(BF)
    for b in range(16):
        for c in range(2):
            out_ref[2 * b + c, :, 0:128] = rows[16 * b : 16 * b + 16, c * 128 : c * 128 + 128]
            out_ref[2 * b + c, :, 128:256] = tails[16 * b : 16 * b + 16, c * 128 : c * 128 + 128]
            out_ref[2 * b + c, :, 256:384] = spread[16 * b : 16 * b + 16, :]


def final_kernel(*refs):
    r_ref, rank_ref, gg_ref, ig_ref, r2_ref, own = refs[:6]
    others = refs[6:13]
    tok_ref, group_ref, inner_ref = refs[13:]
    total = own[...].astype(F32)
    for o in others:
        total += o[...].astype(F32)
    tok_ref[:, 0:128] = total.astype(BF)
    lane = iota((256, 128), 1)
    half = jnp.zeros((256, 128), F32)
    scores = []
    for k in range(2):
        here, left, slot = slot_masks(r_ref, rank_ref, k)
        main = as_bf(here & (left == (slot & 15)))
        tail = as_bf(here & (left == 16 + (slot & 15)) & ((slot & 15) < 4))
        half += mm(main, r2_ref[:, 0:128]) + mm(tail, r2_ref[:, 128:256])
        sc = r2_ref[:, 256:384]
        picked = jnp.where((lane & 3) < 2, mm(main, sc), mm(tail, sc))
        scores.append(jnp.sum(picked, axis=1, keepdims=True))
    tok_ref[:, 128:256] = half.astype(BF)
    gg = gg_ref[...]
    ig = ig_ref[...]
    inner_ref[:, 0:1] = gg * scores[0]
    inner_ref[:, 1:2] = gg * scores[1]
    group_ref[...] = ig[:, 0:1] * scores[0] + ig[:, 1:2] * scores[1]


def sds(shape, dtype=BF):
    return jax.ShapeDtypeStruct(shape, dtype)


def call(kernel, outs, n_in, scalars=True, **kw):
    specs = ([SCALARS] if scalars else []) + [WHOLE] * n_in
    return pl.pallas_call(
        kernel,
        out_shape=outs,
        in_specs=specs,
        out_specs=jax.tree.map(lambda _: WHOLE, outs),
        compiler_params=pltpu.CompilerParams(vmem_limit_bytes=60 * 2**20),
        **kw,
    )


def around(k):
    return [(i, (i + k) % 8) for i in range(8)]


def per_device(tokens, cotangent, routing, group_gate, inner_gate, w_gate, w_up, w_down):
    z = lax.axis_index("z")
    info = jnp.stack([z % 2, lax.axis_index("core"), z]).astype(I32)
    gg = group_gate[:, None]

    swap = [(0, 1), (1, 0)]
    other = [lax.ppermute(w[0], "core", swap) for w in (w_gate, w_up, w_down)]

    whole = lambda i: (0, 0)
    a_send, rank, ohm, oht = pl.pallas_call(
        pack_a,
        grid=(A_UNITS,),
        in_specs=[
            SCALARS,
            pl.BlockSpec((256, 2), whole),
            pl.BlockSpec((256, UNIT), lambda i: (0, i)),
            pl.BlockSpec((256, UNIT), lambda i: (0, i)),
        ],
        out_specs=(
            pl.BlockSpec((256, WIRE), lambda i: (0, i)),
            pl.BlockSpec((256, 128), whole),
            pl.BlockSpec((256, 256), whole),
            pl.BlockSpec((256, 256), whole),
        ),
        out_shape=(sds((256, A_UNITS * WIRE)), sds((256, 128), F32), sds((256, 256)), sds((256, 256))),
    )(info, routing, tokens, cotangent)
    a_recv = lax.all_to_all(a_send.reshape(16, 16, -1), "ep", 0, 0, tiled=True).reshape(256, -1)

    bx, bg, wt = pl.pallas_call(
        pack_b,
        grid=(B_UNITS,),
        in_specs=[
            pl.BlockSpec((256, 2), whole),
            pl.BlockSpec((256, 1), whole),
            pl.BlockSpec((256, 2), whole),
            pl.BlockSpec((256, 256), whole),
            pl.BlockSpec((256, 256), whole),
            pl.BlockSpec((256, UNIT), lambda i: (0, A_UNITS + i)),
            pl.BlockSpec((256, UNIT), lambda i: (0, A_UNITS + i)),
        ],
        out_specs=(
            pl.BlockSpec((256, WIRE), lambda i: (0, i)),
            pl.BlockSpec((256, WIRE), lambda i: (0, i)),
            pl.BlockSpec((256, 128), whole),
        ),
        out_shape=(sds((256, B_UNITS * WIRE)), sds((256, B_UNITS * WIRE)), sds((256, 128))),
    )(routing, gg, inner_gate, ohm, oht, tokens, cotangent)
    b_send = jnp.concatenate([bx, bg, wt], axis=1)
    b_send, a_recv = lax.optimization_barrier((b_send, a_recv))
    z1 = lax.ppermute(a_recv[:128], "z", around(1))
    z2 = lax.ppermute(a_recv[128:], "z", around(-1))
    b_recv = lax.all_to_all(b_send.reshape(16, 16, -1), "ep", 0, 0, tiled=True).reshape(256, -1)
    bw = B_UNITS * WIRE
    wcat = jnp.concatenate([w_gate[0], other[0], w_up[0], other[1]], axis=1)
    wd = jnp.concatenate([w_down[0], other[2]], axis=0)

    outs = (
        sds((320, 4096)), sds((320, 4096)), sds((320, 128), F32), sds((320, 256)),
        sds((320, 256)), sds((320, 256)), sds((32, 16, 2 * WIRE)), sds((8, 336, 256)),
    )
    xs, gs, cw, hid, gown, gpar, p1, p2 = call(expert_kernel, outs, 8)(
        info, a_recv, z1, z2, b_recv[:, :bw], b_recv[:, bw : 2 * bw], b_recv[:, 2 * bw :], wcat, wd
    )

    p2_recv = [lax.ppermute(p2[k], "z", around(k)) for k in range(1, 8)]
    r1 = lax.all_to_all(p1, ("ep", "core"), 0, 0, tiled=True).reshape(512, -1)

    def tdot(a, b):
        return lax.dot_general(a, b, (((0,), (0,)), ((), ())), preferred_element_type=F32)

    scaled = (cw[:, 0:1] * gs).astype(BF)
    gu_par = lax.ppermute(tdot(xs, gpar).astype(BF), "core", swap)
    d_par = lax.ppermute(tdot(hid[:, 128:], scaled).astype(BF), "core", swap)
    gate_grad = (tdot(xs, gown[:, :128]) + gu_par[:, :128]).astype(BF)
    upper_grad = (tdot(xs, gown[:, 128:]) + gu_par[:, 128:]).astype(BF)
    down_grad = (tdot(hid[:, :128], scaled) + d_par).astype(BF)

    pieces = call(combine_kernel, sds((8, 256, 128)), 3, scratch_shapes=[pltpu.VMEM((256, 1024), BF)])(
        info, routing, rank, r1
    )
    q_recv = [lax.ppermute(pieces[k], "z", around(k)) for k in range(1, 8)]
    mid = call(middle_kernel, sds((32, 16, 384)), 8, scalars=False)(p2[0], *p2_recv)
    r2 = lax.all_to_all(mid, ("ep", "core"), 0, 0, tiled=True).reshape(512, 384)
    token_grad, group_grad, inner_grad = call(
        final_kernel, (sds((256, 256)), sds((256, 1), F32), sds((256, 2), F32)), 13, scalars=False
    )(routing, rank, gg, inner_gate, r2, pieces[0], *q_recv)
    return token_grad, group_grad[:, 0], inner_grad, gate_grad[None], upper_grad[None], down_grad[None]


def solution(mesh):
    split = Mesh(mesh.devices.reshape(16, 8, 2), ("ep", "z", "core"))
    tp = ("z", "core")
    return jax.shard_map(
        per_device,
        mesh=split,
        in_specs=(
            P("ep", None), P("ep", None), P("ep", None), P("ep"), P("ep", None),
            P("ep", None, tp), P("ep", None, tp), P("ep", tp, None),
        ),
        out_specs=(
            P("ep", tp), P("ep"), P("ep", None), P("ep", None, tp), P("ep", None, tp), P("ep", tp, None),
        ),
        check_vma=False,
    )
```

```python
import jax
import jax.numpy as jnp
from jax import lax
from jax.experimental import pallas as pl
from jax.experimental.pallas import tpu as pltpu
from jax.sharding import Mesh, PartitionSpec as P


BF = jnp.bfloat16
F32 = jnp.float32
I32 = jnp.int32
UNIT = 512
WIRE = 640
A_UNITS = 5
B_UNITS = 3
WHOLE = pl.BlockSpec(memory_space=pltpu.VMEM)
FAR = pl.BlockSpec(memory_space=pltpu.HBM)
SCALARS = pl.BlockSpec(memory_space=pltpu.SMEM)


def iota(shape, dim):
    return lax.broadcasted_iota(I32, shape, dim)


def as_bf(mask):
    return jnp.where(mask, 1.0, 0.0).astype(BF)


def mm(a, b, ca=1, cb=0):
    return lax.dot_general(a, b, (((ca,), (cb,)), ((), ())), preferred_element_type=F32)


def fold_matrix():
    o = iota((256, 256), 0)
    i = iota((256, 256), 1)
    return as_bf(((o >> 6) == ((i >> 2) & 3)) & (((o >> 2) & 15) == (i >> 4)) & ((o & 3) == (i & 3)))


def expert_rows():
    return as_bf((iota((256, 128), 0) >> 4) == iota((256, 128), 1))


def pack_unit(ohm, oht, src, out):
    row = iota((256, 256), 0)
    out[:, :UNIT] = mm(ohm, src[...]).astype(BF)
    tail = jnp.zeros((256, 128), F32)
    for q in range(4):
        tail += mm(jnp.where(((row >> 2) & 3) == q, oht, jnp.zeros_like(oht)), src[:, q * 128 : q * 128 + 128])
    out[:, UNIT:WIRE] = tail.astype(BF)


def pack_a(s_ref, r_ref, x_ref, g_ref, a_ref, info_ref, ohm_ref, oht_ref, src, dst, sem_in, sem_out):
    def fetch(ref, u):
        return pltpu.make_async_copy(ref.at[:, u * UNIT : (u + 1) * UNIT], src.at[u], sem_in.at[u])

    for u in range(A_UNITS):

        @pl.when(s_ref[0] == 0)
        def _(u=u):
            fetch(x_ref, u).start()

        @pl.when(s_ref[0] != 0)
        def _(u=u):
            fetch(g_ref, u).start()

    r = r_ref[...]
    expert = iota((128, 256), 0)
    named = (r[0:1, :] == expert) | (r[1:2, :] == expert)
    ti = iota((256, 256), 0)
    tj = iota((256, 256), 1)
    rank = mm(as_bf(named), as_bf(ti < tj))
    for k in range(2):
        info_ref[2 * k : 2 * k + 1, :] = r[k : k + 1, :].astype(F32)
        mine = jnp.where(r[k : k + 1, :] == expert, rank, 0.0)
        info_ref[2 * k + 1 : 2 * k + 2, :] = jnp.sum(mine, axis=0, keepdims=True)
    info_ref[4:8, :] = jnp.zeros((4, 256), F32)
    spread = mm(expert_rows(), jnp.where(named, rank, -1.0).astype(BF)).astype(I32)
    first = s_ref[1] * 20
    ohm_ref[...] = as_bf(spread == first + (ti & 15))
    oht_ref[...] = as_bf(spread == first + 16 + (ti & 3))

    outs = []
    for u in range(A_UNITS):
        fetch(x_ref, u).wait()
        pack_unit(ohm_ref[...], oht_ref[...], src.at[u], dst.at[u])
        out = pltpu.make_async_copy(dst.at[u], a_ref.at[:, u * WIRE : (u + 1) * WIRE], sem_out.at[u])
        out.start()
        outs.append(out)
    for out in outs:
        out.wait()


def pack_b(r_ref, gg_ref, ig_ref, info_ref, ohm_ref, oht_ref, x_ref, g_ref, bx_ref, bg_ref, wt_ref, mask_ref):
    ohm = ohm_ref[...]
    oht = oht_ref[...]
    pack_unit(ohm, oht, x_ref, bx_ref)
    pack_unit(ohm, oht, g_ref, bg_ref)

    @pl.when(pl.program_id(0) == 0)
    def _():
        r = r_ref[...]
        expert = iota((128, 256), 0)
        comb = gg_ref[...] * ig_ref[...]
        w = jnp.where(r[0:1, :] == expert, comb[0:1, :], 0.0) + jnp.where(r[1:2, :] == expert, comb[1:2, :], 0.0)
        hi = w.astype(BF)
        lo = (w - hi.astype(F32)).astype(BF)

        def picked(oh, part):
            return jnp.sum(oh.astype(F32) * mm(expert_rows(), part), axis=1, keepdims=True)

        lane = iota((256, 128), 1)
        vals = jnp.where(lane == 0, picked(ohm, hi), 0.0)
        vals = jnp.where(lane == 1, picked(ohm, lo), vals)
        vals = jnp.where(lane == 2, picked(oht, hi), vals)
        vals = jnp.where(lane == 3, picked(oht, lo), vals)
        wt_ref[...] = vals.astype(BF)

        eye = as_bf(iota((256, 256), 0) == iota((256, 256), 1))
        cols = mm(eye, info_ref[...].astype(BF), 1, 1).astype(I32)
        slot = iota((256, 512), 1)
        for k in range(2):
            here = (slot >> 5) == cols[:, 2 * k : 2 * k + 1]
            left = cols[:, 2 * k + 1 : 2 * k + 2] - 20 * ((slot >> 4) & 1)
            mask_ref[k, :, :] = as_bf(here & (left == (slot & 15)))
            mask_ref[2 + k, :, :] = as_bf(here & (left == 16 + (slot & 3)))


def wire(u):
    return slice(u * WIRE, (u + 1) * WIRE)


def cols(u):
    return slice(u * UNIT, (u + 1) * UNIT)


def unpack(fold, buf, dst, u):
    dst[0:256, cols(u)] = buf[:, 0:UNIT]
    t = mm(fold, buf[:, UNIT:WIRE]).astype(BF)
    for q in range(4):
        dst[256:320, u * UNIT + q * 128 : u * UNIT + q * 128 + 128] = t[q * 64 : q * 64 + 64, :]


def expert_kernel(s_ref, a_ref, z1_ref, z2_ref, b_ref, wcat_ref, wd_hbm,
                  x_hbm, g_hbm, c_hbm, hid_hbm, in_hbm, sc_hbm, up_hbm, dn_hbm,
                  buf_a, buf_z, buf_b, wt_buf, wc, wd, xv, gv, pre_acc, gh_acc,
                  c_out, hid_out, in_out, sc_out, up_out, dn_out, sem_i, sem_w, sem_o):
    units = A_UNITS + B_UNITS
    at = 2 * B_UNITS * WIRE
    in_wt = pltpu.make_async_copy(b_ref.at[:, at : at + 128], wt_buf, sem_w.at[2 * units])
    loads = []
    for u in range(units):
        if u < A_UNITS:
            rows = [
                pltpu.make_async_copy(a_ref.at[:, wire(u)], buf_a.at[u], sem_i.at[3 * u]),
                pltpu.make_async_copy(z1_ref.at[:, wire(u)], buf_z.at[u, 0:128], sem_i.at[3 * u + 1]),
                pltpu.make_async_copy(z2_ref.at[:, wire(u)], buf_z.at[u, 128:256], sem_i.at[3 * u + 2]),
            ]
        else:
            n = u - A_UNITS
            m = n + B_UNITS
            rows = [
                pltpu.make_async_copy(b_ref.at[:, wire(n)], buf_b.at[n], sem_i.at[3 * u]),
                pltpu.make_async_copy(b_ref.at[:, wire(m)], buf_b.at[m], sem_i.at[3 * u + 1]),
            ]
        weights = [
            pltpu.make_async_copy(wcat_ref.at[cols(u)], wc.at[cols(u)], sem_w.at[2 * u]),
            pltpu.make_async_copy(wd_hbm.at[:, cols(u)], wd.at[:, cols(u)], sem_w.at[2 * u + 1]),
        ]
        for copy in rows + weights:
            copy.start()
        loads.append((rows, weights))
    in_wt.start()
    outs = []

    def send(src, dst):
        outs.append(pltpu.make_async_copy(src, dst, sem_o.at[len(outs)]))
        outs[-1].start()

    fold = fold_matrix()
    fold0 = fold[0:64, :]
    lane = iota((256, 128), 1)
    for u in range(units):
        for copy in loads[u][0]:
            copy.wait()
        if u < A_UNITS:

            @pl.when(s_ref[0] == 0)
            def _(u=u):
                unpack(fold, buf_a.at[u], xv, u)
                unpack(fold, buf_z.at[u], gv, u)

            @pl.when(s_ref[0] != 0)
            def _(u=u):
                unpack(fold, buf_a.at[u], gv, u)
                unpack(fold, buf_z.at[u], xv, u)
        else:
            unpack(fold, buf_b.at[u - A_UNITS], xv, u)
            unpack(fold, buf_b.at[u - A_UNITS + B_UNITS], gv, u)
        for copy in loads[u][1]:
            copy.wait()
        if u % 2 == 1:
            both = slice((u - 1) * UNIT, (u + 1) * UNIT)
            send(xv.at[:, both], x_hbm.at[:, both])
            send(gv.at[:, both], g_hbm.at[:, both])
            p = mm(xv[:, both], wc[both, :])
            g = mm(gv[:, both], wd[:, both], 1, 1)
            if u > 1:
                p += pre_acc[...]
                g += gh_acc[...]
            pre_acc[...] = p
            gh_acc[...] = g
    in_wt.wait()
    wt = wt_buf[...]
    wt_f = wt.astype(F32)
    c_main = wt_f[:, 0:1] + wt_f[:, 1:2]
    wt_t = mm(fold0, wt)
    c_tail = wt_t[:, 2:3] + wt_t[:, 3:4]

    def activations(at, count, c):
        gate_pre = pre_acc[at : at + count, 0:256]
        up_pre = pre_acc[at : at + count, 256:512]
        g = gh_acc[at : at + count, :]
        sig = jax.nn.sigmoid(gate_pre)
        silu = gate_pre * sig
        hid = (silu * up_pre).astype(BF)
        score = jnp.sum(g * hid.astype(F32), axis=1, keepdims=True)
        weighted = c * g
        in_out[at : at + count, 0:256] = (weighted * up_pre * sig * (1.0 + gate_pre * (1.0 - sig))).astype(BF)
        in_out[at : at + count, 256:512] = (weighted * silu).astype(BF)
        hid_out[at : at + count, :] = hid
        c_out[at : at + count, :] = jnp.broadcast_to(c, (count, 128))
        hi = score.astype(BF).astype(F32)
        return hi, score - hi

    hi_m, lo_m = activations(0, 256, c_main)
    hi_t, lo_t = activations(256, 64, c_tail)
    lane_t = iota((64, 128), 1)
    tails = jnp.where(lane_t == 2, hi_t, jnp.where(lane_t == 3, lo_t, 0.0)).astype(BF)
    vals = jnp.where(lane == 0, hi_m, jnp.where(lane == 1, lo_m, 0.0)) + mm(fold0, tails, 0, 0)
    vals = vals.astype(BF)
    sc_out[...] = vals
    dn_out[0:256, 1024:1152] = vals
    dn_out[256:320, 1024:1152] = jnp.zeros((64, 128), BF)
    send(in_out, in_hbm)
    send(hid_out, hid_hbm)
    send(c_out, c_hbm)
    send(sc_out, sc_hbm)

    ins = in_out[...]
    for i in range(4):
        dst = up_out if i < 2 else dn_out
        for c in range(2):
            at = pl.multiple_of((2 * i + 1 - s_ref[0]) * 512 + c * 256, 256)
            col = (i % 2) * 512 + c * 256
            dst[:, col : col + 256] = mm(ins, wc[pl.ds(at, 256), :], 1, 1).astype(BF)
        if i == 1:
            send(up_out, up_hbm)
    send(dn_out, dn_hbm)
    for copy in outs:
        copy.wait()


def return_kernel(s_ref, in_ref, wcat_ref, sc_ref, up_ref, dn_ref, out_ref):
    fold = fold_matrix()
    ins = in_ref[...]
    lane = iota((256, 128), 1)
    s = sc_ref[...].astype(F32) + dn_ref[0:256, 1024:1152].astype(F32)
    s = s + pltpu.roll(s, 127, 1)
    hi = s.astype(BF).astype(F32)
    vals = jnp.where((lane & 1) == 0, hi, pltpu.roll(s - hi, 1, 1)).astype(BF)
    for c in range(2):
        for u in range(2):
            src = (up_ref, dn_ref)[u]
            tails = []
            for h in range(2):
                at = pl.multiple_of((4 * u + 2 * h + s_ref[0]) * 512 + c * 256, 256)
                col = h * 512 + c * 256
                part = mm(ins, wcat_ref[pl.ds(at, 256), :], 1, 1) + src[0:320, col : col + 256].astype(F32)
                part = part.astype(BF)
                for b in range(16):
                    out_ref[2 * b + c, :, u * WIRE + h * 256 : u * WIRE + h * 256 + 256] = part[16 * b : 16 * b + 16, :]
                tails += [part[256:320, 0:128], part[256:320, 128:256]]
            folded = mm(fold, jnp.concatenate(tails, axis=0), 0, 0).astype(BF)
            for b in range(16):
                out_ref[2 * b + c, :, u * WIRE + UNIT : (u + 1) * WIRE] = folded[16 * b : 16 * b + 16, :]
        for b in range(16):
            out_ref[2 * b + c, :, 2 * WIRE :] = vals[16 * b : 16 * b + 16, :]


def combine_kernel(s_ref, mask_ref, r1_ref, *outs):
    acc_ref = outs[4]
    slot = iota((256, 512), 1)
    zero = jnp.zeros((256, 512), BF)
    main = mask_ref[0] + mask_ref[1]
    tail_any = mask_ref[2] + mask_ref[3]
    tails = [jnp.where(((slot >> 2) & 3) == q, tail_any, zero) for q in range(4)]
    for u in range(2):
        full = mm(main, r1_ref[:, u * WIRE : u * WIRE + UNIT])
        tail = r1_ref[:, u * WIRE + UNIT : (u + 1) * WIRE]
        for q in range(4):
            acc_ref[:, u * UNIT + q * 128 : u * UNIT + q * 128 + 128] = (
                full[:, q * 128 : q * 128 + 128] + mm(tails[q], tail)
            ).astype(BF)
    sc = r1_ref[:, 2 * WIRE :]
    rows = []
    for k in range(2):
        m = mm(sc, mask_ref[k], 0, 1)
        t = mm(sc, jnp.where(((slot >> 2) & 3) == 0, mask_ref[2 + k], zero), 0, 1)
        score = m[0:1, :] + m[1:2, :] + t[2:3, :] + t[3:4, :]
        hi = score.astype(BF).astype(F32)
        rows += [hi, score - hi]
    row16 = iota((16, 256), 0)
    scores = jnp.zeros((16, 256), F32)
    for n in range(4):
        scores = jnp.where(row16 == n, rows[n], scores)
    scores = scores.astype(BF)
    for n in range(4):
        dest = lax.rem(s_ref[2] + 2 * n, 8)
        at = pl.multiple_of((dest >> 1) * 256, 256)
        outs[n][0:256, :] = acc_ref[:, pl.ds(at, 256)]
        outs[n][256:272, :] = scores


def final_kernel(gg_ref, ig_ref, p0, p1, p2, p3, tok_ref, group_ref, inner_ref):
    total = p0[...].astype(F32) + p1[...].astype(F32) + p2[...].astype(F32) + p3[...].astype(F32)
    tok_ref[...] = total[0:256, :].astype(BF)
    s0 = total[256:257, :] + total[257:258, :]
    s1 = total[258:259, :] + total[259:260, :]
    gg = gg_ref[...]
    inner_ref[0:1, :] = gg * s0
    inner_ref[1:2, :] = gg * s1
    group_ref[...] = ig_ref[0:1, :] * s0 + ig_ref[1:2, :] * s1


def sds(shape, dtype=BF):
    return jax.ShapeDtypeStruct(shape, dtype)


def call(kernel, outs, ins, mib, scalars=True, out_specs=None, **kw):
    specs = ([SCALARS] if scalars else []) + list(ins)
    return pl.pallas_call(
        kernel,
        out_shape=outs,
        in_specs=specs,
        out_specs=out_specs or jax.tree.map(lambda _: WHOLE, outs),
        compiler_params=pltpu.CompilerParams(vmem_limit_bytes=mib * 2**20),
        **kw,
    )


def vmem(*shape):
    return pltpu.VMEM(shape, BF)


def sems(n):
    return pltpu.SemaphoreType.DMA((n,))


def around(k):
    return [(i, (i + k) % 8) for i in range(8)]


def tdot(a, b):
    return lax.dot_general(a, b, (((0,), (0,)), ((), ())), preferred_element_type=F32)


def per_device(tokens, cotangent, routing, group_gate, inner_gate, w_gate, w_up, w_down):
    z = lax.axis_index("z")
    info = jnp.stack([z % 2, lax.axis_index("core"), z]).astype(I32)
    gg = group_gate[None, :]
    ig = inner_gate.T
    rt = routing.T

    swap = [(0, 1), (1, 0)]
    other = [lax.ppermute(w[0], "core", swap) for w in (w_gate, w_up, w_down)]

    whole = lambda i: (0, 0)
    block = lambda i: (0, i)
    later = lambda i: (0, A_UNITS + i)
    small = pltpu.CompilerParams(vmem_limit_bytes=12 * 2**20)
    a_send, ranks, ohm, oht = call(
        pack_a,
        (sds((256, A_UNITS * WIRE)), sds((8, 256), F32), sds((256, 256)), sds((256, 256))),
        (WHOLE, FAR, FAR),
        63,
        out_specs=(FAR, WHOLE, WHOLE, WHOLE),
        scratch_shapes=[
            vmem(A_UNITS, 256, UNIT), vmem(A_UNITS, 256, WIRE), sems(A_UNITS), sems(A_UNITS),
        ],
    )(info, rt, tokens, cotangent)
    a_recv = lax.all_to_all(a_send.reshape(16, 16, -1), "ep", 0, 0, tiled=True).reshape(256, -1)

    bx, bg, wt, masks = pl.pallas_call(
        pack_b,
        grid=(B_UNITS,),
        in_specs=[
            pl.BlockSpec((2, 256), whole),
            pl.BlockSpec((1, 256), whole),
            pl.BlockSpec((2, 256), whole),
            pl.BlockSpec((8, 256), whole),
            pl.BlockSpec((256, 256), whole),
            pl.BlockSpec((256, 256), whole),
            pl.BlockSpec((256, UNIT), later),
            pl.BlockSpec((256, UNIT), later),
        ],
        out_specs=(
            pl.BlockSpec((256, WIRE), block),
            pl.BlockSpec((256, WIRE), block),
            pl.BlockSpec((256, 128), whole),
            pl.BlockSpec((4, 256, 512), lambda i: (0, 0, 0)),
        ),
        out_shape=(
            sds((256, B_UNITS * WIRE)), sds((256, B_UNITS * WIRE)), sds((256, 128)), sds((4, 256, 512)),
        ),
        compiler_params=small,
    )(rt, gg, ig, ranks, ohm, oht, tokens, cotangent)
    b_send = jnp.concatenate([bx, bg, wt], axis=1)
    b_send, a_recv = lax.optimization_barrier((b_send, a_recv))
    z1 = lax.ppermute(a_recv[:128], "z", around(1))
    z2 = lax.ppermute(a_recv[128:], "z", around(-1))
    b_recv = lax.all_to_all(b_send.reshape(16, 16, -1), "ep", 0, 0, tiled=True).reshape(256, -1)
    wcat = jnp.concatenate([w_gate[0], other[0], w_up[0], other[1]], axis=1)
    wd = jnp.concatenate([w_down[0], other[2]], axis=0)

    outs = (
        sds((320, 4096)), sds((320, 4096)), sds((320, 128), F32), sds((320, 256)),
        sds((320, 512)), sds((256, 128)), sds((320, 1024)), sds((320, 1152)),
    )
    n = A_UNITS + B_UNITS
    xs, gs, cw, hid, ins, sc, up, dn = call(
        expert_kernel,
        outs,
        (FAR,) * 6,
        63,
        out_specs=(FAR,) * 8,
        scratch_shapes=[
            vmem(A_UNITS, 256, WIRE), vmem(A_UNITS, 256, WIRE), vmem(2 * B_UNITS, 256, WIRE), vmem(256, 128),
            vmem(4096, 512), vmem(256, 4096), vmem(320, 4096), vmem(320, 4096),
            pltpu.VMEM((320, 512), F32), pltpu.VMEM((320, 256), F32),
            pltpu.VMEM((320, 128), F32), vmem(320, 256), vmem(320, 512), vmem(256, 128),
            vmem(320, 1024), vmem(320, 1152), sems(3 * n), sems(2 * n + 1), sems(n + 6),
        ],
    )(info, a_recv, z1, z2, b_recv, wcat, wd)
    up = lax.ppermute(up, "z", around(1))
    dn = lax.ppermute(dn, "z", around(-1))

    scaled = (cw[:, 0:1] * gs).astype(BF)
    d_par = tdot(hid[:, 128:], scaled).astype(BF)
    g_par = tdot(xs, ins[:, 128:256]).astype(BF)
    u_par = tdot(xs, ins[:, 384:512]).astype(BF)
    d_par, g_par, u_par = [lax.ppermute(t, "core", swap) for t in (d_par, g_par, u_par)]

    p1 = call(return_kernel, sds((32, 16, 2 * WIRE + 128)), (WHOLE,) * 5, 8)(info, ins, wcat, sc, up, dn)
    r1 = lax.all_to_all(p1, ("ep", "core"), 0, 0, tiled=True).reshape(512, -1)

    down_grad = (tdot(hid[:, :128], scaled) + d_par).astype(BF)
    gate_grad = (tdot(xs, ins[:, 0:128]) + g_par).astype(BF)
    upper_grad = (tdot(xs, ins[:, 256:384]) + u_par).astype(BF)

    pieces = call(
        combine_kernel, (sds((272, 256)),) * 4, (WHOLE,) * 2, 8, scratch_shapes=[pltpu.VMEM((256, 1024), BF)]
    )(info, masks, r1)
    got = [lax.ppermute(pieces[n], "z", around(2 * n)) for n in (2, 1, 3)]
    token_grad, group_grad, inner_grad = call(
        final_kernel, (sds((256, 256)), sds((1, 256), F32), sds((2, 256), F32)), (WHOLE,) * 6, 4, scalars=False
    )(gg, ig, pieces[0], *got)
    return token_grad, group_grad[0], inner_grad.T, gate_grad[None], upper_grad[None], down_grad[None]


def solution(mesh):
    split = Mesh(mesh.devices.reshape(16, 8, 2), ("ep", "z", "core"))
    tp = ("z", "core")
    return jax.shard_map(
        per_device,
        mesh=split,
        in_specs=(
            P("ep", None), P("ep", None), P("ep", None), P("ep"), P("ep", None),
            P("ep", None, tp), P("ep", None, tp), P("ep", tp, None),
        ),
        out_specs=(
            P("ep", tp), P("ep"), P("ep", None), P("ep", None, tp), P("ep", None, tp), P("ep", tp, None),
        ),
        check_vma=False,
    )
```

```python
import jax
import jax.numpy as jnp
from jax import lax
from jax.experimental import pallas as pl
from jax.experimental.pallas import tpu as pltpu
from jax.sharding import Mesh, PartitionSpec as P


BF = jnp.bfloat16
F32 = jnp.float32
I32 = jnp.int32
UNIT = 512
WIRE = 640
A_UNITS = 5
B_UNITS = 3
WHOLE = pl.BlockSpec(memory_space=pltpu.VMEM)
FAR = pl.BlockSpec(memory_space=pltpu.HBM)


def z_index():
    return lax.axis_index("z")


def parity():
    return lax.rem(z_index(), 2)


def iota(shape, dim):
    return lax.broadcasted_iota(I32, shape, dim)


def as_bf(mask):
    return jnp.where(mask, 1.0, 0.0).astype(BF)


def mm(a, b, ca=1, cb=0):
    return lax.dot_general(a, b, (((ca,), (cb,)), ((), ())), preferred_element_type=F32)


def fold_matrix():
    o = iota((256, 256), 0)
    i = iota((256, 256), 1)
    return as_bf(((o >> 6) == ((i >> 2) & 3)) & (((o >> 2) & 15) == (i >> 4)) & ((o & 3) == (i & 3)))


def expert_rows():
    return as_bf((iota((256, 128), 0) >> 4) == iota((256, 128), 1))


def pack_unit(ohm, oht, fold, src, out):
    out[:, :UNIT] = mm(ohm, src[...]).astype(BF)
    t = mm(oht, src[...]).astype(BF)
    t = jnp.concatenate([t[:, q * 128 : q * 128 + 128] for q in range(4)], axis=0)
    out[:, UNIT:WIRE] = mm(fold, t, 0, 0).astype(BF)


def pack_a(r_hbm, x_ref, g_ref, a_ref, info_hbm, ohm_hbm, oht_hbm,
           r_ref, info_ref, ohm_ref, oht_ref, src, dst, sem_in, sem_out):
    par = parity()
    get_r = pltpu.make_async_copy(r_hbm, r_ref, sem_in.at[A_UNITS])
    get_r.start()

    def fetch(ref, u):
        return pltpu.make_async_copy(ref.at[:, u * UNIT : (u + 1) * UNIT], src.at[u], sem_in.at[u])

    for u in range(A_UNITS):

        @pl.when(par == 0)
        def _(u=u):
            fetch(x_ref, u).start()

        @pl.when(par != 0)
        def _(u=u):
            fetch(g_ref, u).start()

    get_r.wait()
    r = r_ref[...]
    expert = iota((128, 256), 0)
    named = (r[0:1, :] == expert) | (r[1:2, :] == expert)
    ti = iota((256, 256), 0)
    tj = iota((256, 256), 1)
    rank = mm(as_bf(named), as_bf(ti < tj))
    for k in range(2):
        info_ref[2 * k : 2 * k + 1, :] = r[k : k + 1, :].astype(F32)
        mine = jnp.where(r[k : k + 1, :] == expert, rank, 0.0)
        info_ref[2 * k + 1 : 2 * k + 2, :] = jnp.sum(mine, axis=0, keepdims=True)
    info_ref[4:8, :] = jnp.zeros((4, 256), F32)
    spread = mm(expert_rows(), jnp.where(named, rank, -1.0).astype(BF)).astype(I32)
    first = lax.axis_index("core") * 20
    ohm_ref[...] = as_bf(spread == first + (ti & 15))
    row64 = iota((64, 128), 0)
    by_expert = jnp.where(named, rank, -1.0).astype(BF)
    tail_spread = mm(as_bf((row64 >> 2) == iota((64, 128), 1)), by_expert).astype(I32)
    oht_ref[...] = as_bf(tail_spread == first + 16 + (iota((64, 256), 0) & 3))
    fold = fold_matrix()
    outs = []
    for n, (ref, hbm) in enumerate(((info_ref, info_hbm), (ohm_ref, ohm_hbm), (oht_ref, oht_hbm))):
        outs.append(pltpu.make_async_copy(ref, hbm, sem_out.at[A_UNITS + n]))
        outs[-1].start()
    for u in range(A_UNITS):
        fetch(x_ref, u).wait()
        pack_unit(ohm_ref[...], oht_ref[...], fold, src.at[u], dst.at[u])
        out = pltpu.make_async_copy(dst.at[u], a_ref.at[:, u * WIRE : (u + 1) * WIRE], sem_out.at[u])
        out.start()
        outs.append(out)
    for out in outs:
        out.wait()


def pack_b(r_ref, gg_ref, ig_ref, info_ref, ohm_ref, oht_ref, x_ref, g_ref, bx_ref, bg_ref, wt_ref, mask_ref):
    ohm = ohm_ref[...]
    oht = oht_ref[...]
    fold = fold_matrix()
    pack_unit(ohm, oht, fold, x_ref, bx_ref)
    pack_unit(ohm, oht, fold, g_ref, bg_ref)

    @pl.when(pl.program_id(0) == 0)
    def _():
        r = r_ref[...]
        expert = iota((128, 256), 0)
        comb = gg_ref[...] * ig_ref[...]
        w = jnp.where(r[0:1, :] == expert, comb[0:1, :], 0.0) + jnp.where(r[1:2, :] == expert, comb[1:2, :], 0.0)
        hi = w.astype(BF)
        lo = (w - hi.astype(F32)).astype(BF)

        def picked(oh, rows, part):
            return jnp.sum(oh.astype(F32) * mm(rows, part), axis=1, keepdims=True)

        lane = iota((256, 128), 1)
        lane64 = iota((64, 128), 1)
        rows64 = as_bf((iota((64, 128), 0) >> 2) == lane64)
        tails = jnp.where(lane64 == 2, picked(oht, rows64, hi), 0.0)
        tails = jnp.where(lane64 == 3, picked(oht, rows64, lo), tails).astype(BF)
        vals = jnp.where(lane == 0, picked(ohm, expert_rows(), hi), mm(fold[0:64, :], tails, 0, 0))
        vals = jnp.where(lane == 1, picked(ohm, expert_rows(), lo), vals)
        wt_ref[...] = vals.astype(BF)

        eye = as_bf(iota((256, 256), 0) == iota((256, 256), 1))
        cols = mm(eye, info_ref[...].astype(BF), 1, 1).astype(I32)
        slot = iota((256, 512), 1)
        for k in range(2):
            here = (slot >> 5) == cols[:, 2 * k : 2 * k + 1]
            left = cols[:, 2 * k + 1 : 2 * k + 2] - 20 * ((slot >> 4) & 1)
            mask_ref[k, :, :] = as_bf(here & (left == (slot & 15)))
            mask_ref[2 + k, :, :] = as_bf(here & (left == 16 + (slot & 3)))


def wire(u):
    return slice(u * WIRE, (u + 1) * WIRE)


def cols(u):
    return slice(u * UNIT, (u + 1) * UNIT)


def place_tail(dst, u, t):
    for q in range(4):
        dst[256:320, u * UNIT + q * 128 : u * UNIT + q * 128 + 128] = t[q * 64 : q * 64 + 64, :]


def unpack(fold, buf, dst, u):
    dst[0:256, cols(u)] = buf[:, 0:UNIT]
    place_tail(dst, u, mm(fold, buf[:, UNIT:WIRE]).astype(BF))


def expert_kernel(a_ref, z1_ref, z2_ref, b_ref, wcat_ref, wd_hbm,
                  c_hbm, hid_hbm, in_hbm, sc_hbm, up_hbm, dn_hbm,
                  buf_a, buf_z, buf_b, wt_buf, wc, wd, xv, gv, pre_acc, gh_acc,
                  c_out, hid_out, in_out, sc_out, up_out, dn_out, sem_i, sem_w, sem_o):
    par = parity()
    units = A_UNITS + B_UNITS
    at = 2 * B_UNITS * WIRE
    in_wt = pltpu.make_async_copy(b_ref.at[:, at : at + 128], wt_buf, sem_w.at[2 * units])
    loads = []
    for u in range(units):
        if u < A_UNITS:
            rows = [
                pltpu.make_async_copy(a_ref.at[:, wire(u)], buf_a.at[u], sem_i.at[3 * u]),
                pltpu.make_async_copy(z1_ref.at[:, wire(u)], buf_z.at[u, 0:128], sem_i.at[3 * u + 1]),
                pltpu.make_async_copy(z2_ref.at[:, wire(u)], buf_z.at[u, 128:256], sem_i.at[3 * u + 2]),
            ]
        else:
            n = u - A_UNITS
            m = n + B_UNITS
            rows = [
                pltpu.make_async_copy(b_ref.at[:, wire(n)], buf_b.at[n], sem_i.at[3 * u]),
                pltpu.make_async_copy(b_ref.at[:, wire(m)], buf_b.at[m], sem_i.at[3 * u + 1]),
            ]
        weights = [
            pltpu.make_async_copy(wcat_ref.at[cols(u)], wc.at[cols(u)], sem_w.at[2 * u]),
            pltpu.make_async_copy(wd_hbm.at[:, cols(u)], wd.at[:, cols(u)], sem_w.at[2 * u + 1]),
        ]
        for copy in rows + weights:
            copy.start()
        loads.append((rows, weights))
    in_wt.start()
    outs = []

    def send(src, dst):
        outs.append(pltpu.make_async_copy(src, dst, sem_o.at[len(outs)]))
        outs[-1].start()

    fold = fold_matrix()
    fold0 = fold[0:64, :]
    lane = iota((256, 128), 1)
    for u in range(units):
        for copy in loads[u][0]:
            copy.wait()
        if u < A_UNITS:

            @pl.when(par == 0)
            def _(u=u):
                unpack(fold, buf_a.at[u], xv, u)
                unpack(fold, buf_z.at[u], gv, u)

            @pl.when(par != 0)
            def _(u=u):
                unpack(fold, buf_a.at[u], gv, u)
                unpack(fold, buf_z.at[u], xv, u)
        else:
            unpack(fold, buf_b.at[u - A_UNITS], xv, u)
            unpack(fold, buf_b.at[u - A_UNITS + B_UNITS], gv, u)
        for copy in loads[u][1]:
            copy.wait()
        if u % 2 == 1:
            both = slice((u - 1) * UNIT, (u + 1) * UNIT)
            p = mm(xv[:, both], wc[both, :])
            g = mm(gv[:, both], wd[:, both], 1, 1)
            if u > 1:
                p += pre_acc[...]
                g += gh_acc[...]
            pre_acc[...] = p
            gh_acc[...] = g
    in_wt.wait()
    wt = wt_buf[...]
    wt_f = wt.astype(F32)
    c_main = wt_f[:, 0:1] + wt_f[:, 1:2]
    wt_t = mm(fold0, wt)
    c_tail = wt_t[:, 2:3] + wt_t[:, 3:4]

    def activations(at, count, c):
        gate_pre = pre_acc[at : at + count, 0:256]
        up_pre = pre_acc[at : at + count, 256:512]
        g = gh_acc[at : at + count, :]
        sig = jax.nn.sigmoid(gate_pre)
        silu = gate_pre * sig
        hid = (silu * up_pre).astype(BF)
        score = jnp.sum(g * hid.astype(F32), axis=1, keepdims=True)
        weighted = c * g
        in_out[at : at + count, 0:256] = (weighted * up_pre * sig * (1.0 + gate_pre * (1.0 - sig))).astype(BF)
        in_out[at : at + count, 256:512] = (weighted * silu).astype(BF)
        hid_out[at : at + count, :] = hid
        c_out[at : at + count, :] = jnp.broadcast_to(c, (count, 128))
        hi = score.astype(BF).astype(F32)
        return hi, score - hi

    hi_m, lo_m = activations(0, 256, c_main)
    hi_t, lo_t = activations(256, 64, c_tail)
    lane_t = iota((64, 128), 1)
    tails = jnp.where(lane_t == 2, hi_t, jnp.where(lane_t == 3, lo_t, 0.0)).astype(BF)
    vals = jnp.where(lane == 0, hi_m, jnp.where(lane == 1, lo_m, 0.0)) + mm(fold0, tails, 0, 0)
    vals = vals.astype(BF)
    sc_out[...] = vals
    dn_out[0:256, 1024:1152] = vals
    dn_out[256:320, 1024:1152] = jnp.zeros((64, 128), BF)
    send(in_out, in_hbm)
    send(hid_out, hid_hbm)
    send(c_out, c_hbm)
    send(sc_out, sc_hbm)

    ins = in_out[...]
    for i in range(4):
        dst = up_out if i < 2 else dn_out
        for c in range(2):
            at = pl.multiple_of((2 * i + 1 - par) * 512 + c * 256, 256)
            col = (i % 2) * 512 + c * 256
            dst[:, col : col + 256] = mm(ins, wc[pl.ds(at, 256), :], 1, 1).astype(BF)
        if i == 1:
            send(up_out, up_hbm)
    send(dn_out, dn_hbm)
    for copy in outs:
        copy.wait()


def rows_kernel(a_ref, z1_ref, z2_ref, b_ref, x_out, g_out):
    par = parity()
    fold = fold_matrix()

    def from_z(dst, u):
        dst[0:128, cols(u)] = z1_ref[:, u * WIRE : u * WIRE + UNIT]
        dst[128:256, cols(u)] = z2_ref[:, u * WIRE : u * WIRE + UNIT]
        at = slice(u * WIRE + UNIT, (u + 1) * WIRE)
        place_tail(dst, u, mm(fold, jnp.concatenate([z1_ref[:, at], z2_ref[:, at]], axis=0)).astype(BF))

    @pl.when(par == 0)
    def _():
        for u in range(A_UNITS):
            unpack(fold, a_ref.at[:, wire(u)], x_out, u)
            from_z(g_out, u)

    @pl.when(par != 0)
    def _():
        for u in range(A_UNITS):
            unpack(fold, a_ref.at[:, wire(u)], g_out, u)
            from_z(x_out, u)

    for n in range(B_UNITS):
        unpack(fold, b_ref.at[:, wire(n)], x_out, A_UNITS + n)
        unpack(fold, b_ref.at[:, wire(B_UNITS + n)], g_out, A_UNITS + n)


def return_kernel(in_ref, wcat_ref, sc_ref, up_ref, dn_ref, out_ref):
    par = parity()
    fold = fold_matrix()
    ins = in_ref[...]
    lane = iota((256, 128), 1)
    s = sc_ref[...].astype(F32) + dn_ref[0:256, 1024:1152].astype(F32)
    s = s + pltpu.roll(s, 127, 1)
    hi = s.astype(BF).astype(F32)
    vals = jnp.where((lane & 1) == 0, hi, pltpu.roll(s - hi, 1, 1)).astype(BF)
    for c in range(2):
        for u in range(2):
            src = (up_ref, dn_ref)[u]
            tails = []
            for h in range(2):
                at = pl.multiple_of((4 * u + 2 * h + par) * 512 + c * 256, 256)
                col = h * 512 + c * 256
                part = mm(ins, wcat_ref[pl.ds(at, 256), :], 1, 1) + src[0:320, col : col + 256].astype(F32)
                part = part.astype(BF)
                for b in range(16):
                    out_ref[2 * b + c, :, u * WIRE + h * 256 : u * WIRE + h * 256 + 256] = part[16 * b : 16 * b + 16, :]
                tails += [part[256:320, 0:128], part[256:320, 128:256]]
            folded = mm(fold, jnp.concatenate(tails, axis=0), 0, 0).astype(BF)
            for b in range(16):
                out_ref[2 * b + c, :, u * WIRE + UNIT : (u + 1) * WIRE] = folded[16 * b : 16 * b + 16, :]
        for b in range(16):
            out_ref[2 * b + c, :, 2 * WIRE :] = vals[16 * b : 16 * b + 16, :]


def combine_kernel(mask_ref, r1_ref, *outs):
    acc_ref = outs[4]
    slot = iota((256, 512), 1)
    zero = jnp.zeros((256, 512), BF)
    main = mask_ref[0] + mask_ref[1]
    tail_any = mask_ref[2] + mask_ref[3]
    tails = [jnp.where(((slot >> 2) & 3) == q, tail_any, zero) for q in range(4)]
    for u in range(2):
        full = mm(main, r1_ref[:, u * WIRE : u * WIRE + UNIT])
        tail = r1_ref[:, u * WIRE + UNIT : (u + 1) * WIRE]
        for q in range(4):
            acc_ref[:, u * UNIT + q * 128 : u * UNIT + q * 128 + 128] = (
                full[:, q * 128 : q * 128 + 128] + mm(tails[q], tail)
            ).astype(BF)
    sc = r1_ref[:, 2 * WIRE :]
    rows = []
    for k in range(2):
        m = mm(sc, mask_ref[k], 0, 1)
        t = mm(sc, jnp.where(((slot >> 2) & 3) == 0, mask_ref[2 + k], zero), 0, 1)
        score = m[0:1, :] + m[1:2, :] + t[2:3, :] + t[3:4, :]
        hi = score.astype(BF).astype(F32)
        rows += [hi, score - hi]
    row16 = iota((16, 256), 0)
    scores = jnp.zeros((16, 256), F32)
    for n in range(4):
        scores = jnp.where(row16 == n, rows[n], scores)
    scores = scores.astype(BF)
    for n in range(4):
        dest = lax.rem(z_index() + 2 * n, 8)
        at = pl.multiple_of((dest >> 1) * 256, 256)
        outs[n][0:256, :] = acc_ref[:, pl.ds(at, 256)]
        outs[n][256:272, :] = scores


def final_kernel(gg_ref, ig_ref, p0, p1, p2, p3, tok_ref, group_ref, inner_ref):
    total = p0[...].astype(F32) + p1[...].astype(F32) + p2[...].astype(F32) + p3[...].astype(F32)
    tok_ref[...] = total[0:256, :].astype(BF)
    s0 = total[256:257, :] + total[257:258, :]
    s1 = total[258:259, :] + total[259:260, :]
    gg = gg_ref[...]
    inner_ref[0:1, :] = gg * s0
    inner_ref[1:2, :] = gg * s1
    group_ref[...] = ig_ref[0:1, :] * s0 + ig_ref[1:2, :] * s1


def sds(shape, dtype=BF):
    return jax.ShapeDtypeStruct(shape, dtype)


def call(kernel, outs, ins, mib, out_specs=None, **kw):
    return pl.pallas_call(
        kernel,
        out_shape=outs,
        in_specs=list(ins),
        out_specs=out_specs or jax.tree.map(lambda _: WHOLE, outs),
        compiler_params=pltpu.CompilerParams(vmem_limit_bytes=mib * 2**20),
        **kw,
    )


def vmem(*shape):
    return pltpu.VMEM(shape, BF)


def sems(n):
    return pltpu.SemaphoreType.DMA((n,))


def around(k):
    return [(i, (i + k) % 8) for i in range(8)]


def tdot(a, b):
    return lax.dot_general(a, b, (((0,), (0,)), ((), ())), preferred_element_type=F32)


def per_device(tokens, cotangent, routing, group_gate, inner_gate, w_gate, w_up, w_down):
    gg = group_gate[None, :]
    ig = inner_gate.T
    rt = routing.T

    swap = [(0, 1), (1, 0)]
    other = [lax.ppermute(w[0], "core", swap) for w in (w_gate, w_up, w_down)]

    whole = lambda i: (0, 0)
    block = lambda i: (0, i)
    later = lambda i: (0, A_UNITS + i)
    small = pltpu.CompilerParams(vmem_limit_bytes=12 * 2**20)
    a_send, ranks, ohm, oht = call(
        pack_a,
        (sds((256, A_UNITS * WIRE)), sds((8, 256), F32), sds((256, 256)), sds((64, 256))),
        (FAR,) * 3,
        63,
        out_specs=(FAR,) * 4,
        scratch_shapes=[
            pltpu.VMEM((2, 256), I32), pltpu.VMEM((8, 256), F32), vmem(256, 256), vmem(64, 256),
            vmem(A_UNITS, 256, UNIT), vmem(A_UNITS, 256, WIRE), sems(A_UNITS + 1), sems(A_UNITS + 3),
        ],
    )(rt, tokens, cotangent)
    a_recv = lax.all_to_all(a_send.reshape(16, 16, -1), "ep", 0, 0, tiled=True).reshape(256, -1)

    bx, bg, wt, masks = pl.pallas_call(
        pack_b,
        grid=(B_UNITS,),
        in_specs=[
            pl.BlockSpec((2, 256), whole),
            pl.BlockSpec((1, 256), whole),
            pl.BlockSpec((2, 256), whole),
            pl.BlockSpec((8, 256), whole),
            pl.BlockSpec((256, 256), whole),
            pl.BlockSpec((64, 256), whole),
            pl.BlockSpec((256, UNIT), later),
            pl.BlockSpec((256, UNIT), later),
        ],
        out_specs=(
            pl.BlockSpec((256, WIRE), block),
            pl.BlockSpec((256, WIRE), block),
            pl.BlockSpec((256, 128), whole),
            pl.BlockSpec((4, 256, 512), lambda i: (0, 0, 0)),
        ),
        out_shape=(
            sds((256, B_UNITS * WIRE)), sds((256, B_UNITS * WIRE)), sds((256, 128)), sds((4, 256, 512)),
        ),
        compiler_params=small,
    )(rt, gg, ig, ranks, ohm, oht, tokens, cotangent)
    b_send = jnp.concatenate([bx, bg, wt], axis=1)
    b_send, a_recv = lax.optimization_barrier((b_send, a_recv))
    z1 = lax.ppermute(a_recv[:128], "z", around(1))
    z2 = lax.ppermute(a_recv[128:], "z", around(-1))
    b_recv = lax.all_to_all(b_send.reshape(16, 16, -1), "ep", 0, 0, tiled=True).reshape(256, -1)
    wcat = jnp.concatenate([w_gate[0], other[0], w_up[0], other[1]], axis=1)
    wd = jnp.concatenate([w_down[0], other[2]], axis=0)

    outs = (
        sds((320, 128), F32), sds((320, 256)), sds((320, 512)), sds((256, 128)), sds((320, 1024)), sds((320, 1152)),
    )
    n = A_UNITS + B_UNITS
    cw, hid, ins, sc, up, dn = call(
        expert_kernel,
        outs,
        (FAR,) * 6,
        63,
        out_specs=(FAR,) * 6,
        scratch_shapes=[
            vmem(A_UNITS, 256, WIRE), vmem(A_UNITS, 256, WIRE), vmem(2 * B_UNITS, 256, WIRE), vmem(256, 128),
            vmem(4096, 512), vmem(256, 4096), vmem(320, 4096), vmem(320, 4096),
            pltpu.VMEM((320, 512), F32), pltpu.VMEM((320, 256), F32),
            pltpu.VMEM((320, 128), F32), vmem(320, 256), vmem(320, 512), vmem(256, 128),
            vmem(320, 1024), vmem(320, 1152), sems(3 * n), sems(2 * n + 1), sems(6),
        ],
    )(a_recv, z1, z2, b_recv, wcat, wd)
    up = lax.ppermute(up, "z", around(1))
    dn = lax.ppermute(dn, "z", around(-1))

    xs, gs = call(rows_kernel, (sds((320, 4096)),) * 2, (WHOLE,) * 4, 50)(a_recv, z1, z2, b_recv)

    scaled = (cw[:, 0:1] * gs).astype(BF)
    d_par = tdot(hid[:, 128:], scaled).astype(BF)
    g_par = tdot(xs, ins[:, 128:256]).astype(BF)
    u_par = tdot(xs, ins[:, 384:512]).astype(BF)
    d_par, g_par, u_par = [lax.ppermute(t, "core", swap) for t in (d_par, g_par, u_par)]

    p1 = call(return_kernel, sds((32, 16, 2 * WIRE + 128)), (WHOLE,) * 5, 8)(ins, wcat, sc, up, dn)
    r1 = lax.all_to_all(p1, ("ep", "core"), 0, 0, tiled=True).reshape(512, -1)

    down_grad = (tdot(hid[:, :128], scaled) + d_par).astype(BF)
    gate_grad = (tdot(xs, ins[:, 0:128]) + g_par).astype(BF)
    upper_grad = (tdot(xs, ins[:, 256:384]) + u_par).astype(BF)

    pieces = call(
        combine_kernel, (sds((272, 256)),) * 4, (WHOLE,) * 2, 8, scratch_shapes=[pltpu.VMEM((256, 1024), BF)]
    )(masks, r1)
    got = [lax.ppermute(pieces[n], "z", around(2 * n)) for n in (2, 1, 3)]
    token_grad, group_grad, inner_grad = call(
        final_kernel, (sds((256, 256)), sds((1, 256), F32), sds((2, 256), F32)), (WHOLE,) * 6, 4
    )(gg, ig, pieces[0], *got)
    return token_grad, group_grad[0], inner_grad.T, gate_grad[None], upper_grad[None], down_grad[None]


def solution(mesh):
    split = Mesh(mesh.devices.reshape(16, 8, 2), ("ep", "z", "core"))
    tp = ("z", "core")
    return jax.shard_map(
        per_device,
        mesh=split,
        in_specs=(
            P("ep", None), P("ep", None), P("ep", None), P("ep"), P("ep", None),
            P("ep", None, tp), P("ep", None, tp), P("ep", tp, None),
        ),
        out_specs=(
            P("ep", tp), P("ep"), P("ep", None), P("ep", None, tp), P("ep", None, tp), P("ep", tp, None),
        ),
        check_vma=False,
    )
```

```python
import jax
import jax.numpy as jnp
from jax import lax
from jax.experimental import pallas as pl
from jax.experimental.pallas import tpu as pltpu
from jax.sharding import Mesh, PartitionSpec as P


BF = jnp.bfloat16
F32 = jnp.float32
I32 = jnp.int32
UNIT = 512
WIRE = 640
A_UNITS = 5
B_UNITS = 3
WHOLE = pl.BlockSpec(memory_space=pltpu.VMEM)
FAR = pl.BlockSpec(memory_space=pltpu.HBM)


def z_index():
    return lax.axis_index("z")


def parity():
    return lax.rem(z_index(), 2)


def iota(shape, dim):
    return lax.broadcasted_iota(I32, shape, dim)


def as_bf(mask):
    return jnp.where(mask, 1.0, 0.0).astype(BF)


def mm(a, b, ca=1, cb=0):
    return lax.dot_general(a, b, (((ca,), (cb,)), ((), ())), preferred_element_type=F32)


def fold_matrix():
    o = iota((256, 256), 0)
    i = iota((256, 256), 1)
    return as_bf(((o >> 6) == ((i >> 2) & 3)) & (((o >> 2) & 15) == (i >> 4)) & ((o & 3) == (i & 3)))


def expert_rows():
    return as_bf((iota((256, 128), 0) >> 4) == iota((256, 128), 1))


def pack_unit(ohm, oht, fold, src, out):
    out[:, :UNIT] = mm(ohm, src[...]).astype(BF)
    t = mm(oht, src[...]).astype(BF)
    t = jnp.concatenate([t[:, q * 128 : q * 128 + 128] for q in range(4)], axis=0)
    out[:, UNIT:WIRE] = mm(fold, t, 0, 0).astype(BF)


def pack_a(r_hbm, x_ref, g_ref, a_ref, info_hbm, ohm_hbm, oht_hbm,
           r_ref, info_ref, ohm_ref, oht_ref, src, dst, sem_in, sem_out):
    par = parity()
    get_r = pltpu.make_async_copy(r_hbm, r_ref, sem_in.at[A_UNITS])
    get_r.start()

    def fetch(ref, u):
        return pltpu.make_async_copy(ref.at[:, u * UNIT : (u + 1) * UNIT], src.at[u], sem_in.at[u])

    for u in range(A_UNITS):

        @pl.when(par == 0)
        def _(u=u):
            fetch(x_ref, u).start()

        @pl.when(par != 0)
        def _(u=u):
            fetch(g_ref, u).start()

    get_r.wait()
    r = r_ref[...]
    expert = iota((128, 256), 0)
    named = (r[0:1, :] == expert) | (r[1:2, :] == expert)
    ti = iota((256, 256), 0)
    tj = iota((256, 256), 1)
    rank = mm(as_bf(named), as_bf(ti < tj))
    for k in range(2):
        info_ref[2 * k : 2 * k + 1, :] = r[k : k + 1, :].astype(F32)
        mine = jnp.where(r[k : k + 1, :] == expert, rank, 0.0)
        info_ref[2 * k + 1 : 2 * k + 2, :] = jnp.sum(mine, axis=0, keepdims=True)
    info_ref[4:8, :] = jnp.zeros((4, 256), F32)
    spread = mm(expert_rows(), jnp.where(named, rank, -1.0).astype(BF)).astype(I32)
    first = lax.axis_index("core") * 20
    ohm_ref[...] = as_bf(spread == first + (ti & 15))
    row64 = iota((64, 128), 0)
    by_expert = jnp.where(named, rank, -1.0).astype(BF)
    tail_spread = mm(as_bf((row64 >> 2) == iota((64, 128), 1)), by_expert).astype(I32)
    oht_ref[...] = as_bf(tail_spread == first + 16 + (iota((64, 256), 0) & 3))
    fold = fold_matrix()
    outs = []
    for n, (ref, hbm) in enumerate(((info_ref, info_hbm), (ohm_ref, ohm_hbm), (oht_ref, oht_hbm))):
        outs.append(pltpu.make_async_copy(ref, hbm, sem_out.at[A_UNITS + n]))
        outs[-1].start()
    for u in range(A_UNITS):
        fetch(x_ref, u).wait()
        pack_unit(ohm_ref[...], oht_ref[...], fold, src.at[u], dst.at[u])
        out = pltpu.make_async_copy(dst.at[u], a_ref.at[:, u * WIRE : (u + 1) * WIRE], sem_out.at[u])
        out.start()
        outs.append(out)
    for out in outs:
        out.wait()


def pack_b(r_ref, gg_ref, ig_ref, info_ref, ohm_ref, oht_ref, x_ref, g_ref, bx_ref, bg_ref, wt_ref, mask_ref):
    ohm = ohm_ref[...]
    oht = oht_ref[...]
    fold = fold_matrix()
    pack_unit(ohm, oht, fold, x_ref, bx_ref)
    pack_unit(ohm, oht, fold, g_ref, bg_ref)

    @pl.when(pl.program_id(0) == 0)
    def _():
        r = r_ref[...]
        expert = iota((128, 256), 0)
        comb = gg_ref[...] * ig_ref[...]
        w = jnp.where(r[0:1, :] == expert, comb[0:1, :], 0.0) + jnp.where(r[1:2, :] == expert, comb[1:2, :], 0.0)
        hi = w.astype(BF)
        lo = (w - hi.astype(F32)).astype(BF)

        def picked(oh, rows, part):
            return jnp.sum(oh.astype(F32) * mm(rows, part), axis=1, keepdims=True)

        lane = iota((256, 128), 1)
        lane64 = iota((64, 128), 1)
        rows64 = as_bf((iota((64, 128), 0) >> 2) == lane64)
        tails = jnp.where(lane64 == 2, picked(oht, rows64, hi), 0.0)
        tails = jnp.where(lane64 == 3, picked(oht, rows64, lo), tails).astype(BF)
        vals = jnp.where(lane == 0, picked(ohm, expert_rows(), hi), mm(fold[0:64, :], tails, 0, 0))
        vals = jnp.where(lane == 1, picked(ohm, expert_rows(), lo), vals)
        wt_ref[...] = vals.astype(BF)

        eye = as_bf(iota((256, 256), 0) == iota((256, 256), 1))
        cols = mm(eye, info_ref[...].astype(BF), 1, 1).astype(I32)
        slot = iota((256, 512), 1)
        for k in range(2):
            here = (slot >> 5) == cols[:, 2 * k : 2 * k + 1]
            left = cols[:, 2 * k + 1 : 2 * k + 2] - 20 * ((slot >> 4) & 1)
            mask_ref[k, :, :] = as_bf(here & (left == (slot & 15)))
            mask_ref[2 + k, :, :] = as_bf(here & (left == 16 + (slot & 3)))


def wire(u):
    return slice(u * WIRE, (u + 1) * WIRE)


def cols(u):
    return slice(u * UNIT, (u + 1) * UNIT)


def place_tail(dst, u, t):
    for q in range(4):
        dst[256:320, u * UNIT + q * 128 : u * UNIT + q * 128 + 128] = t[q * 64 : q * 64 + 64, :]


def unpack(fold, buf, dst, u):
    dst[0:256, cols(u)] = buf[:, 0:UNIT]
    place_tail(dst, u, mm(fold, buf[:, UNIT:WIRE]).astype(BF))


def expert_kernel(a_ref, z1_ref, z2_ref, b_ref, wcat_ref, wd_hbm,
                  c_hbm, hid_hbm, in_hbm, sc_hbm, up_hbm, dn_hbm,
                  buf_a, buf_z, buf_b, wt_buf, wc, wd, xv, gv, pre_acc, gh_acc,
                  c_out, hid_out, in_out, sc_out, up_out, dn_out, sem_i, sem_w, sem_o):
    par = parity()
    units = A_UNITS + B_UNITS
    at = 2 * B_UNITS * WIRE
    in_wt = pltpu.make_async_copy(b_ref.at[:, at : at + 128], wt_buf, sem_w.at[2 * units])
    loads = []
    for u in range(units):
        if u < A_UNITS:
            rows = [
                pltpu.make_async_copy(a_ref.at[:, wire(u)], buf_a.at[u], sem_i.at[3 * u]),
                pltpu.make_async_copy(z1_ref.at[:, wire(u)], buf_z.at[u, 0:128], sem_i.at[3 * u + 1]),
                pltpu.make_async_copy(z2_ref.at[:, wire(u)], buf_z.at[u, 128:256], sem_i.at[3 * u + 2]),
            ]
        else:
            n = u - A_UNITS
            m = n + B_UNITS
            rows = [
                pltpu.make_async_copy(b_ref.at[:, wire(n)], buf_b.at[n], sem_i.at[3 * u]),
                pltpu.make_async_copy(b_ref.at[:, wire(m)], buf_b.at[m], sem_i.at[3 * u + 1]),
            ]
        weights = [
            pltpu.make_async_copy(wcat_ref.at[cols(u)], wc.at[cols(u)], sem_w.at[2 * u]),
            pltpu.make_async_copy(wd_hbm.at[:, cols(u)], wd.at[:, cols(u)], sem_w.at[2 * u + 1]),
        ]
        for copy in rows + weights:
            copy.start()
        loads.append((rows, weights))
    in_wt.start()
    outs = []

    def send(src, dst):
        outs.append(pltpu.make_async_copy(src, dst, sem_o.at[len(outs)]))
        outs[-1].start()

    fold = fold_matrix()
    fold0 = fold[0:64, :]
    lane = iota((256, 128), 1)
    for u in range(units):
        for copy in loads[u][0]:
            copy.wait()
        if u < A_UNITS:

            @pl.when(par == 0)
            def _(u=u):
                unpack(fold, buf_a.at[u], xv, u)
                unpack(fold, buf_z.at[u], gv, u)

            @pl.when(par != 0)
            def _(u=u):
                unpack(fold, buf_a.at[u], gv, u)
                unpack(fold, buf_z.at[u], xv, u)
        else:
            unpack(fold, buf_b.at[u - A_UNITS], xv, u)
            unpack(fold, buf_b.at[u - A_UNITS + B_UNITS], gv, u)
        for copy in loads[u][1]:
            copy.wait()
        if u % 2 == 1:
            both = slice((u - 1) * UNIT, (u + 1) * UNIT)
            p = mm(xv[:, both], wc[both, :])
            g = mm(gv[:, both], wd[:, both], 1, 1)
            if u > 1:
                p += pre_acc[...]
                g += gh_acc[...]
            pre_acc[...] = p
            gh_acc[...] = g
    in_wt.wait()
    wt = wt_buf[...]
    wt_f = wt.astype(F32)
    c_main = wt_f[:, 0:1] + wt_f[:, 1:2]
    wt_t = mm(fold0, wt)
    c_tail = wt_t[:, 2:3] + wt_t[:, 3:4]

    def activations(at, count, c):
        gate_pre = pre_acc[at : at + count, 0:256]
        up_pre = pre_acc[at : at + count, 256:512]
        g = gh_acc[at : at + count, :]
        sig = jax.nn.sigmoid(gate_pre)
        silu = gate_pre * sig
        hid = (silu * up_pre).astype(BF)
        score = jnp.sum(g * hid.astype(F32), axis=1, keepdims=True)
        weighted = c * g
        in_out[at : at + count, 0:256] = (weighted * up_pre * sig * (1.0 + gate_pre * (1.0 - sig))).astype(BF)
        in_out[at : at + count, 256:512] = (weighted * silu).astype(BF)
        hid_out[at : at + count, :] = hid
        c_out[at : at + count, :] = jnp.broadcast_to(c, (count, 128))
        hi = score.astype(BF).astype(F32)
        return hi, score - hi

    hi_m, lo_m = activations(0, 256, c_main)
    hi_t, lo_t = activations(256, 64, c_tail)
    lane_t = iota((64, 128), 1)
    tails = jnp.where(lane_t == 2, hi_t, jnp.where(lane_t == 3, lo_t, 0.0)).astype(BF)
    vals = jnp.where(lane == 0, hi_m, jnp.where(lane == 1, lo_m, 0.0)) + mm(fold0, tails, 0, 0)
    vals = vals.astype(BF)
    sc_out[...] = vals
    dn_out[0:256, 1024:1152] = vals
    dn_out[256:320, 1024:1152] = jnp.zeros((64, 128), BF)
    send(in_out, in_hbm)
    send(hid_out, hid_hbm)
    send(c_out, c_hbm)
    send(sc_out, sc_hbm)

    ins = in_out[...]
    for i in range(4):
        dst = up_out if i < 2 else dn_out
        for c in range(2):
            at = pl.multiple_of((2 * i + 1 - par) * 512 + c * 256, 256)
            col = (i % 2) * 512 + c * 256
            dst[:, col : col + 256] = mm(ins, wc[pl.ds(at, 256), :], 1, 1).astype(BF)
        if i == 1:
            send(up_out, up_hbm)
    send(dn_out, dn_hbm)
    for copy in outs:
        copy.wait()


def rows_kernel(a_ref, z1_ref, z2_ref, b_ref, x_out, g_out):
    par = parity()
    fold = fold_matrix()

    def from_z(dst, u):
        dst[0:128, cols(u)] = z1_ref[:, u * WIRE : u * WIRE + UNIT]
        dst[128:256, cols(u)] = z2_ref[:, u * WIRE : u * WIRE + UNIT]
        at = slice(u * WIRE + UNIT, (u + 1) * WIRE)
        place_tail(dst, u, mm(fold, jnp.concatenate([z1_ref[:, at], z2_ref[:, at]], axis=0)).astype(BF))

    @pl.when(par == 0)
    def _():
        for u in range(A_UNITS):
            unpack(fold, a_ref.at[:, wire(u)], x_out, u)
            from_z(g_out, u)

    @pl.when(par != 0)
    def _():
        for u in range(A_UNITS):
            unpack(fold, a_ref.at[:, wire(u)], g_out, u)
            from_z(x_out, u)

    for n in range(B_UNITS):
        unpack(fold, b_ref.at[:, wire(n)], x_out, A_UNITS + n)
        unpack(fold, b_ref.at[:, wire(B_UNITS + n)], g_out, A_UNITS + n)


def return_kernel(in_ref, wcat_ref, sc_ref, up_ref, dn_ref, out_ref):
    par = parity()
    fold = fold_matrix()
    ins = in_ref[...]
    lane = iota((256, 128), 1)
    s = sc_ref[...].astype(F32) + dn_ref[0:256, 1024:1152].astype(F32)
    s = s + pltpu.roll(s, 127, 1)
    hi = s.astype(BF).astype(F32)
    vals = jnp.where((lane & 1) == 0, hi, pltpu.roll(s - hi, 1, 1)).astype(BF)
    for c in range(2):
        for u in range(2):
            src = (up_ref, dn_ref)[u]
            tails = []
            for h in range(2):
                at = pl.multiple_of((4 * u + 2 * h + par) * 512 + c * 256, 256)
                col = h * 512 + c * 256
                part = mm(ins, wcat_ref[pl.ds(at, 256), :], 1, 1) + src[0:320, col : col + 256].astype(F32)
                part = part.astype(BF)
                for b in range(16):
                    out_ref[2 * b + c, :, u * WIRE + h * 256 : u * WIRE + h * 256 + 256] = part[16 * b : 16 * b + 16, :]
                tails += [part[256:320, 0:128], part[256:320, 128:256]]
            folded = mm(fold, jnp.concatenate(tails, axis=0), 0, 0).astype(BF)
            for b in range(16):
                out_ref[2 * b + c, :, u * WIRE + UNIT : (u + 1) * WIRE] = folded[16 * b : 16 * b + 16, :]
        for b in range(16):
            out_ref[2 * b + c, :, 2 * WIRE :] = vals[16 * b : 16 * b + 16, :]


def combine_kernel(mask_ref, r1_ref, *outs):
    acc_ref = outs[4]
    slot = iota((256, 512), 1)
    zero = jnp.zeros((256, 512), BF)
    main = mask_ref[0] + mask_ref[1]
    tail_any = mask_ref[2] + mask_ref[3]
    tails = [jnp.where(((slot >> 2) & 3) == q, tail_any, zero) for q in range(4)]
    for u in range(2):
        full = mm(main, r1_ref[:, u * WIRE : u * WIRE + UNIT])
        tail = r1_ref[:, u * WIRE + UNIT : (u + 1) * WIRE]
        for q in range(4):
            acc_ref[:, u * UNIT + q * 128 : u * UNIT + q * 128 + 128] = (
                full[:, q * 128 : q * 128 + 128] + mm(tails[q], tail)
            ).astype(BF)
    sc = r1_ref[:, 2 * WIRE :]
    rows = []
    for k in range(2):
        m = mm(sc, mask_ref[k], 0, 1)
        t = mm(sc, jnp.where(((slot >> 2) & 3) == 0, mask_ref[2 + k], zero), 0, 1)
        score = m[0:1, :] + m[1:2, :] + t[2:3, :] + t[3:4, :]
        hi = score.astype(BF).astype(F32)
        rows += [hi, score - hi]
    row8 = iota((8, 256), 0)
    scores = jnp.zeros((8, 256), F32)
    for n in range(4):
        scores = jnp.where(row8 == n, rows[n], scores)
    scores = scores.astype(BF)
    for n in range(4):
        dest = lax.rem(z_index() + 2 * n, 8)
        at = pl.multiple_of((dest >> 1) * 256, 256)
        outs[n][0:256, :] = acc_ref[:, pl.ds(at, 256)]
        outs[n][256:264, :] = scores


def final_kernel(gg_ref, ig_ref, p0, p1, p2, p3, tok_ref, group_ref, inner_ref):
    total = p0[...].astype(F32) + p1[...].astype(F32) + p2[...].astype(F32) + p3[...].astype(F32)
    tok_ref[...] = total[0:256, :].astype(BF)
    s0 = total[256:257, :] + total[257:258, :]
    s1 = total[258:259, :] + total[259:260, :]
    gg = gg_ref[...]
    inner_ref[0:1, :] = gg * s0
    inner_ref[1:2, :] = gg * s1
    group_ref[...] = ig_ref[0:1, :] * s0 + ig_ref[1:2, :] * s1


def sds(shape, dtype=BF):
    return jax.ShapeDtypeStruct(shape, dtype)


def call(kernel, outs, ins, mib, out_specs=None, **kw):
    return pl.pallas_call(
        kernel,
        out_shape=outs,
        in_specs=list(ins),
        out_specs=out_specs or jax.tree.map(lambda _: WHOLE, outs),
        compiler_params=pltpu.CompilerParams(vmem_limit_bytes=mib * 2**20),
        **kw,
    )


def vmem(*shape):
    return pltpu.VMEM(shape, BF)


def sems(n):
    return pltpu.SemaphoreType.DMA((n,))


def around(k):
    return [(i, (i + k) % 8) for i in range(8)]


def tdot(a, b):
    return lax.dot_general(a, b, (((0,), (0,)), ((), ())), preferred_element_type=F32)


def per_device(tokens, cotangent, routing, group_gate, inner_gate, w_gate, w_up, w_down):
    gg = group_gate[None, :]
    ig = inner_gate.T
    rt = routing.T

    swap = [(0, 1), (1, 0)]
    other = [lax.ppermute(w[0], "core", swap) for w in (w_gate, w_up, w_down)]

    whole = lambda i: (0, 0)
    block = lambda i: (0, i)
    later = lambda i: (0, A_UNITS + i)
    small = pltpu.CompilerParams(vmem_limit_bytes=62 * 2**20)
    a_send, ranks, ohm, oht = call(
        pack_a,
        (sds((256, A_UNITS * WIRE)), sds((8, 256), F32), sds((256, 256)), sds((64, 256))),
        (FAR,) * 3,
        63,
        out_specs=(FAR,) * 4,
        scratch_shapes=[
            pltpu.VMEM((2, 256), I32), pltpu.VMEM((8, 256), F32), vmem(256, 256), vmem(64, 256),
            vmem(A_UNITS, 256, UNIT), vmem(A_UNITS, 256, WIRE), sems(A_UNITS + 1), sems(A_UNITS + 3),
        ],
    )(rt, tokens, cotangent)
    a_recv = lax.all_to_all(a_send.reshape(16, 16, -1), "ep", 0, 0, tiled=True).reshape(256, -1)

    bx, bg, wt, masks = pl.pallas_call(
        pack_b,
        grid=(B_UNITS,),
        in_specs=[
            pl.BlockSpec((2, 256), whole),
            pl.BlockSpec((1, 256), whole),
            pl.BlockSpec((2, 256), whole),
            pl.BlockSpec((8, 256), whole),
            pl.BlockSpec((256, 256), whole),
            pl.BlockSpec((64, 256), whole),
            pl.BlockSpec((256, UNIT), later),
            pl.BlockSpec((256, UNIT), later),
        ],
        out_specs=(
            pl.BlockSpec((256, WIRE), block),
            pl.BlockSpec((256, WIRE), block),
            pl.BlockSpec((256, 128), whole),
            pl.BlockSpec((4, 256, 512), lambda i: (0, 0, 0)),
        ),
        out_shape=(
            sds((256, B_UNITS * WIRE)), sds((256, B_UNITS * WIRE)), sds((256, 128)), sds((4, 256, 512)),
        ),
        compiler_params=small,
    )(rt, gg, ig, ranks, ohm, oht, tokens, cotangent)
    b_send = jnp.concatenate([bx, bg, wt], axis=1)
    b_send, a_recv = lax.optimization_barrier((b_send, a_recv))
    z1 = lax.ppermute(a_recv[:128], "z", around(1))
    z2 = lax.ppermute(a_recv[128:], "z", around(-1))
    b_recv = lax.all_to_all(b_send.reshape(16, 16, -1), "ep", 0, 0, tiled=True).reshape(256, -1)
    wcat = jnp.concatenate([w_gate[0], other[0], w_up[0], other[1]], axis=1)
    wd = jnp.concatenate([w_down[0], other[2]], axis=0)

    outs = (
        sds((320, 128), F32), sds((320, 256)), sds((320, 512)), sds((256, 128)), sds((320, 1024)), sds((320, 1152)),
    )
    n = A_UNITS + B_UNITS
    cw, hid, ins, sc, up, dn = call(
        expert_kernel,
        outs,
        (FAR,) * 6,
        63,
        out_specs=(FAR,) * 6,
        scratch_shapes=[
            vmem(A_UNITS, 256, WIRE), vmem(A_UNITS, 256, WIRE), vmem(2 * B_UNITS, 256, WIRE), vmem(256, 128),
            vmem(4096, 512), vmem(256, 4096), vmem(320, 4096), vmem(320, 4096),
            pltpu.VMEM((320, 512), F32), pltpu.VMEM((320, 256), F32),
            pltpu.VMEM((320, 128), F32), vmem(320, 256), vmem(320, 512), vmem(256, 128),
            vmem(320, 1024), vmem(320, 1152), sems(3 * n), sems(2 * n + 1), sems(6),
        ],
    )(a_recv, z1, z2, b_recv, wcat, wd)
    up = lax.ppermute(up, "z", around(1))
    dn = lax.ppermute(dn, "z", around(-1))

    xs, gs = call(rows_kernel, (sds((320, 4096)),) * 2, (WHOLE,) * 4, 50)(a_recv, z1, z2, b_recv)

    scaled = (cw[:, 0:1] * gs).astype(BF)
    d_par = tdot(hid[:, 128:], scaled).astype(BF)
    g_par = tdot(xs, ins[:, 128:256]).astype(BF)
    u_par = tdot(xs, ins[:, 384:512]).astype(BF)
    d_par, g_par, u_par = [lax.ppermute(t, "core", swap) for t in (d_par, g_par, u_par)]

    p1 = call(return_kernel, sds((32, 16, 2 * WIRE + 128)), (WHOLE,) * 5, 8)(ins, wcat, sc, up, dn)
    r1 = lax.all_to_all(p1, ("ep", "core"), 0, 0, tiled=True).reshape(512, -1)

    down_grad = (tdot(hid[:, :128], scaled) + d_par).astype(BF)
    gate_grad = (tdot(xs, ins[:, 0:128]) + g_par).astype(BF)
    upper_grad = (tdot(xs, ins[:, 256:384]) + u_par).astype(BF)

    pieces = call(
        combine_kernel, (sds((264, 256)),) * 4, (WHOLE,) * 2, 8, scratch_shapes=[pltpu.VMEM((256, 1024), BF)]
    )(masks, r1)
    got = [lax.ppermute(pieces[n], "z", around(2 * n)) for n in (2, 1, 3)]
    token_grad, group_grad, inner_grad = call(
        final_kernel, (sds((256, 256)), sds((1, 256), F32), sds((2, 256), F32)), (WHOLE,) * 6, 4
    )(gg, ig, pieces[0], *got)
    return token_grad, group_grad[0], inner_grad.T, gate_grad[None], upper_grad[None], down_grad[None]


def solution(mesh):
    split = Mesh(mesh.devices.reshape(16, 8, 2), ("ep", "z", "core"))
    tp = ("z", "core")
    return jax.shard_map(
        per_device,
        mesh=split,
        in_specs=(
            P("ep", None), P("ep", None), P("ep", None), P("ep"), P("ep", None),
            P("ep", None, tp), P("ep", None, tp), P("ep", tp, None),
        ),
        out_specs=(
            P("ep", tp), P("ep"), P("ep", None), P("ep", None, tp), P("ep", None, tp), P("ep", tp, None),
        ),
        check_vma=False,
    )
```
